768 devices in a mesh: sp: 384 (over z, y, x), tp: 2 (over core).
Axes of the slice: x: 4, y: 8, z: 12, core: 2. Of those that a mesh axis runs over, the one named last changes fastest.
Arguments:
- value_in: bfloat16 [98304, 2048], P('sp', 'tp'), may hold values from -25 to 25, as said below
- gate_in: bfloat16 [98304, 2048], P('sp', 'tp'), may hold values from -6 to 6
- taps: float32 [31, 2048], P(None, 'tp'), may hold values from -1 to 1
- gain: float32 [2048], P('tp'), may hold values from 0.1 to 1.9
- shift: float32 [2048], P('tp'), may hold values from -3 to 3
- w_out: bfloat16 [2048, 2048], P('tp'), may hold values from -0.125 to 0.125
- grad_out: bfloat16 [98304, 2048], P('sp'), may hold values from -6 to 6
Outputs:
- d_value: bfloat16 [98304, 2048], P('sp', 'tp')
- d_gate: bfloat16 [98304, 2048], P('sp', 'tp')
- d_taps: float32 [31, 2048], P(None, 'tp')
- d_gain: float32 [2048], P('tp')
- d_shift: float32 [2048], P('tp')
The draws below stay inside these ranges and needn't reach their ends.
Inputs may be any that keep to these rules, and one draw needn't show every extreme that they name: `value_in`: channel blocks of different magnitude.
All inputs are finite; a program needn't handle non-finite values.
Results may differ from the reference program's by a relative error of at most 0.007.
Values may be sent and summed in bfloat16 or wider, within the bound.
A program may use at most 64 MiB of HBM per device.

```python
import math
import jax
import jax.numpy as jnp
from jax import lax

C = 2048
D = 2048
KERNEL = 31
TOK_DEV = 256
TOKENS = 98304
N_SP = 384


def draw_value_in(key, part):
    key_base = jax.random.fold_in(key, 11)
    key_group = jax.random.fold_in(key, 12)
    key_flip = jax.random.fold_in(key, 13)
    base = jnp.clip(jax.random.normal(key_base, (TOKENS, C), jnp.float32), -4.0, 4.0)
    column = jnp.exp(jax.random.uniform(key_group, (C,), jnp.float32, -0.7, 0.7))
    flip = jax.random.randint(key_flip, (), 0, 2)
    upper = (jnp.arange(C) >= C // 2).astype(jnp.int32)
    factor = jnp.where(upper == flip, 3.0, 1.0)
    return (base * column * factor).astype(jnp.bfloat16)


def shard_levels(own_key, extent, pieces, low, high):
    factor_of = 1.0
    for position, shards_of in pieces:
        heights = jax.random.uniform(jax.random.fold_in(jax.random.fold_in(own_key, 6), position), (shards_of,), jnp.float32, low / len(pieces), high / len(pieces))
        factor_of = factor_of * jnp.repeat(jnp.exp(heights), extent[position] // shards_of).reshape((-1,) + (1,) * (len(extent) - 1 - position))
    return factor_of


def noise(rng, extent, scale, most, pieces=(), kind=jnp.bfloat16):
    array = scale * jax.random.normal(rng, extent, jnp.float32)
    if pieces:
        array = array * shard_levels(rng, extent, pieces, -0.22, 0.18)
    return jnp.clip(array, -most, most).astype(kind)


def setup_inputs(seed: int = 0) -> dict:
    splits = jax.random.split(jax.random.key(seed), 8)
    return {
        "value_in": draw_value_in(jax.random.fold_in(splits[7], 71), 0),
        "gate_in": noise(splits[1], (TOKENS, C), 1.5, 6.0, ((0, 384), (1, 2))),
        "taps": noise(splits[2], (KERNEL, C), 0.18, 1.0, ((1, 2),), jnp.float32),
        "gain": jnp.clip(1.0 + 0.18 * jax.random.normal(splits[3], (C,), jnp.float32), 0.1, 1.9),
        "shift": noise(splits[4], (C,), 0.5, 3.0, ((0, 2),), jnp.float32),
        "w_out": noise(splits[5], (C, D), D ** -0.5, 0.125, ((0, 2),)),
        "grad_out": noise(splits[6], (TOKENS, D), 1.0, 6.0, ((0, 384),)),
    }


EPS = 1e-05

def convolve(window, taps, count):
    total = jnp.zeros((count, window.shape[1]), jnp.float32)
    for offset in range(taps.shape[0]):
        total = total + taps[offset] * window[offset:offset + count]
    return total

def norm_backward(conv_out, grad_rows, gain, shift, w_out):
    width = conv_out.shape[1]
    mean = lax.optimization_barrier(jnp.sum(conv_out, 1)) / width
    var = lax.optimization_barrier(jnp.sum(conv_out * conv_out, 1)) / width - mean * mean
    inv = lax.rsqrt(var + EPS)
    normed = (conv_out - mean[:, None]) * inv[:, None]
    pre = normed * gain + shift
    grad_mix = jnp.dot(grad_rows, w_out.T, preferred_element_type=jnp.float32)
    sig = jax.nn.sigmoid(pre)
    grad_pre = grad_mix * sig * (1.0 + pre * (1.0 - sig))
    grad_normed = grad_pre * gain
    first = lax.optimization_barrier(jnp.sum(grad_normed, 1)) / width
    second = lax.optimization_barrier(jnp.sum(grad_normed * normed, 1)) / width
    grad_conv = inv[:, None] * (grad_normed - first[:, None] - normed * second[:, None])
    return (grad_conv, grad_pre, normed)

def reference(value_in, gate_in, taps, gain, shift, w_out, grad_out):
    half = KERNEL // 2
    gate_sig = jax.nn.sigmoid(gate_in.astype(jnp.float32))
    gated = (value_in.astype(jnp.float32) * gate_sig).astype(jnp.bfloat16)
    gated_pad = jnp.pad(gated, ((half, half), (0, 0)))

    def first_pass(index):
        start = (index * TOK_DEV).astype(jnp.int32)
        window = lax.dynamic_slice_in_dim(gated_pad, start, TOK_DEV + 2 * half, 0).astype(jnp.float32)
        conv_out = convolve(window, taps, TOK_DEV)
        grad_rows = lax.dynamic_slice_in_dim(grad_out, start, TOK_DEV, 0)
        grad_conv, grad_pre, normed = norm_backward(conv_out, grad_rows, gain, shift, w_out)
        return (grad_conv, lax.optimization_barrier(jnp.sum(grad_pre * normed, 0)), lax.optimization_barrier(jnp.sum(grad_pre, 0)))
    blocks = jnp.arange(N_SP, dtype=jnp.int32)
    grad_conv, gain_parts, shift_parts = lax.map(first_pass, blocks)
    grad_conv = grad_conv.reshape(TOKENS, C)
    grad_pad = jnp.pad(grad_conv, ((half, half), (0, 0)))

    def second_pass(index):
        start = (index * TOK_DEV).astype(jnp.int32)
        window = lax.dynamic_slice_in_dim(gated_pad, start, TOK_DEV + 2 * half, 0).astype(jnp.float32)
        grad_win = lax.dynamic_slice_in_dim(grad_pad, start, TOK_DEV + 2 * half, 0)
        own = grad_win[half:half + TOK_DEV]
        grad_gated = jnp.zeros((TOK_DEV, C), jnp.float32)
        for offset in range(KERNEL):
            grad_gated = grad_gated + taps[offset] * grad_win[2 * half - offset:2 * half - offset + TOK_DEV]
        tap_terms = jnp.stack([lax.optimization_barrier(jnp.sum(own * window[offset:offset + TOK_DEV], 0)) for offset in range(KERNEL)])
        return (grad_gated, tap_terms)
    grad_gated, tap_parts = lax.map(second_pass, blocks)
    grad_gated = grad_gated.reshape(TOKENS, C)
    scale = 1.0 / math.sqrt(TOKENS)
    d_value = (grad_gated * gate_sig).astype(jnp.bfloat16)
    d_gate = (grad_gated * value_in.astype(jnp.float32) * gate_sig * (1.0 - gate_sig)).astype(jnp.bfloat16)
    d_taps = lax.optimization_barrier(jnp.sum(tap_parts, 0)) * scale
    d_gain = lax.optimization_barrier(jnp.sum(gain_parts, 0)) * scale
    d_shift = lax.optimization_barrier(jnp.sum(shift_parts, 0)) * scale
    return (d_value, d_gate, d_taps, d_gain, d_shift)
```

```python
import functools
import math

import jax
import jax.numpy as jnp
from jax import lax
from jax.experimental import pallas as pl
from jax.experimental.pallas import tpu as pltpu
from jax.sharding import Mesh
from jax.sharding import PartitionSpec as P

SP = ("sp_0", "sp_1", "sp_2")
EPS = 1e-05
F32 = jnp.float32
BF16 = jnp.bfloat16
MESH = pl.DeviceIdType.MESH

ROWS, WIDTH, KERNEL, HALF = 256, 1024, 31, 15
LANES, SUB, STEPS, PITCH, OUT_PITCH = 8, 8, 32, 72, 40
GROUP = 8


def position(dims):
    nz, ny, nx = dims
    z, y, x = (lax.axis_index(a) for a in SP)
    return z, y, x, lax.axis_index("tp"), (z * ny + y) * nx + x


def place(index, dims):
    nz, ny, nx = dims
    return {"sp_0": index // (ny * nx), "sp_1": (index // nx) % ny, "sp_2": index % nx}


def sigmoid(v):
    return jax.nn.sigmoid(v)


def kernel(
    dims,
    total,
    value_hbm, gate_hbm, taps_hbm, gain_hbm, shift_hbm, w_hbm, cot_hbm,
    d_value_hbm, d_gate_hbm, d_taps_hbm, d_gain_hbm, d_shift_hbm,
    value, gate, taps, gain, shift, w, cot,
    gated, conv, mix, grad, wide, back, parts, bits,
    edge_out, edge_in, tail_out, tail_in,
    stat_out, stat_in, mean_b, inv_b, first_b, second_b,
    tiles, tiles_in, line, final, shift_x, shift_y, shift_z, spare,
    d_value, d_gate, d_taps, d_gain, d_shift,
    in_sem, w_sem, edge_send, edge_recv, stat_send, stat_recv, tail_send, tail_recv,
    rs_send, rs_recv, z_send, z_recv, ag_send, ag_recv, sh_send, sh_recv, out_sem,
):
    nz, ny, nx = dims
    z, y, x, t, me = position(dims)
    n_sp = nz * ny * nx
    plane = ny * nx
    mine = x * ny + y
    after = place(lax.rem(me + 1, n_sp), dims)
    before = place(lax.rem(me + n_sp - 1, n_sp), dims)
    partner = {"tp": 1 - t}

    def in_plane(step):
        q = lax.rem(mine + step, plane)
        return q, {"sp_1": lax.rem(q, ny), "sp_2": q // ny}

    def along(axis, here, count, step):
        q = lax.rem(here + step, count)
        return q, {axis: q}

    barrier = pltpu.get_barrier_semaphore()

    def greet(device):
        pl.semaphore_signal(barrier, inc=1, device_id=device, device_id_type=MESH)

    greet(after)
    greet(before)
    greet(partner)

    @pl.loop(1, nz)
    def _(step):
        greet(along("sp_0", z, nz, step)[1])

    @pl.loop(1, plane)
    def _(step):
        greet(in_plane(step)[1])

    small = [
        pltpu.make_async_copy(src, dst, in_sem.at[i])
        for i, (src, dst) in enumerate(
            [(value_hbm, value), (gate_hbm, gate), (taps_hbm, taps), (gain_hbm, gain),
             (shift_hbm, shift), (cot_hbm, cot)]
        )
    ]
    big = [
        pltpu.make_async_copy(
            w_hbm.at[pl.ds(256 * i, 256)], w.at[pl.ds(256 * i, 256)], w_sem.at[i]
        )
        for i in range(4)
    ]
    small[0].start()
    small[1].start()
    small[5].start()
    for copy in big:
        copy.start()
    for i in (2, 3, 4):
        small[i].start()

    small[0].wait()
    small[1].wait()

    def gated_of(rows, lanes):
        sig = sigmoid(gate[rows, lanes].astype(F32))
        return (value[rows, lanes].astype(F32) * sig).astype(BF16)

    for i, start in enumerate((0, ROWS - 16)):
        edge_out[i] = gated_of(pl.ds(start, 16), slice(None))

    @pl.loop(0, SUB)
    def _(s):
        for half in range(2):
            rows = pl.ds(pl.multiple_of(32 * s + 16 * half, 16), 16)
            for l in range(LANES):
                v = gated_of(rows, slice(128 * l, 128 * l + 128)).astype(F32)
                own = pl.multiple_of(PITCH * (s + 1) + 16 + 16 * half, 8)
                gated[l, pl.ds(own, 16)] = v
                other = pl.multiple_of(PITCH * s + 48 if half == 0 else PITCH * (s + 2), 8)
                gated[l, pl.ds(other, 16)] = v

    small[5].wait()
    for i in range(4):
        big[i].wait()
        for part in range(2):
            l = 2 * i + part
            product = lax.dot_general(
                cot[...], w[pl.ds(128 * l, 128)], (((1,), (1,)), ((), ())),
                preferred_element_type=F32,
            )
            for s in range(SUB):
                mix[l, pl.ds(OUT_PITCH * s, 32)] = product[32 * s : 32 * s + 32]

    for i in (2, 3, 4):
        small[i].wait()

    pl.semaphore_wait(barrier, (nz - 1) + (plane - 1) + 3)

    def exchange(source, target, send, recv, device):
        return pltpu.make_async_remote_copy(
            src_ref=source, dst_ref=target, send_sem=send, recv_sem=recv,
            device_id=device, device_id_type=MESH,
        )

    edges = [
        exchange(edge_out.at[0], edge_in.at[1], edge_send.at[0], edge_recv.at[1], before),
        exchange(edge_out.at[1], edge_in.at[0], edge_send.at[1], edge_recv.at[0], after),
    ]
    for copy in edges:
        copy.start()
    for copy in edges:
        copy.wait()
    absent = (me == 0, me == n_sp - 1)
    for i, start in enumerate((PITCH, SUB * PITCH + 48)):
        for l in range(LANES):
            v = edge_in[i, :, 128 * l : 128 * l + 128].astype(F32)
            gated[l, pl.ds(start, 16)] = jnp.where(absent[i], 0.0, v)

    def tap(k, l):
        lanes = pl.ds(pl.multiple_of(128 * l, 128), 128)
        return jnp.broadcast_to(taps[pl.ds(k, 1), lanes], (SUB, 128))

    @pl.loop(0, LANES)
    def _(l):
        for j0 in range(0, STEPS, GROUP):
            window = [
                gated[l, pl.ds(PITCH + j0 + 1 + i, SUB, stride=PITCH)]
                for i in range(GROUP + KERNEL - 1)
            ]
            sums = [jnp.zeros((SUB, 128), F32)] * GROUP
            for k in range(KERNEL):
                weight = tap(k, l)
                for i in range(GROUP):
                    sums[i] = sums[i] + weight * window[i + k]
            for i in range(GROUP):
                conv[l, pl.ds(8 * (j0 + i), 8)] = sums[i]

    lane = lax.broadcasted_iota(jnp.int32, (SUB, 128), 1)
    zero = jnp.zeros((SUB, 128), F32)

    def at_row(j):
        return pl.ds(pl.multiple_of(8 * j, 8), 8)

    def put(packed, j, v):
        return jnp.where(lane == j, jnp.sum(v, 1, keepdims=True), packed)

    def of_pair(slot):
        copy = exchange(
            stat_out.at[slot], stat_in.at[slot], stat_send.at[slot], stat_recv.at[slot], partner
        )
        copy.start()
        copy.wait()
        return (
            stat_out[slot, 0] + stat_in[slot, 0],
            stat_out[slot, 1] + stat_in[slot, 1],
        )

    def spread(packed, target):
        for j in range(STEPS):
            target[8 * j : 8 * j + 8] = jnp.broadcast_to(packed[:, j : j + 1], (SUB, 128))

    def totals(j, carry):
        one, two = zero, zero
        for l in range(LANES):
            v = conv[l, at_row(j)]
            one = one + v
            two = two + v * v
        return put(carry[0], j, one), put(carry[1], j, two)

    one, two = lax.fori_loop(0, STEPS, totals, (zero, zero))
    stat_out[0, 0] = one
    stat_out[0, 1] = two
    one, two = of_pair(0)
    width = 2.0 * WIDTH
    mean = one / width
    inv = lax.rsqrt(two / width - mean * mean + EPS)
    spread(mean, mean_b)
    spread(inv, inv_b)

    def norm(j, carry):
        packed_one, packed_two, by_gain, by_shift = carry
        by_gain, by_shift = list(by_gain), list(by_shift)
        mean, inv = mean_b[at_row(j)], inv_b[at_row(j)]
        one, two = zero, zero
        for l in range(LANES):
            lanes = slice(128 * l, 128 * l + 128)
            g = gain[:, lanes]
            normed = (conv[l, at_row(j)] - mean) * inv
            pre = normed * g + shift[:, lanes]
            sig = sigmoid(pre)
            grad_pre = mix[l, pl.ds(j, SUB, stride=OUT_PITCH)] * sig * (1.0 + pre * (1.0 - sig))
            grad_normed = grad_pre * g
            one = one + grad_normed
            two = two + grad_normed * normed
            by_gain[l] = by_gain[l] + grad_pre * normed
            by_shift[l] = by_shift[l] + grad_pre
            conv[l, at_row(j)] = normed
            grad[l, at_row(j)] = grad_normed
        return (
            put(packed_one, j, one), put(packed_two, j, two), tuple(by_gain), tuple(by_shift)
        )

    one, two, by_gain, by_shift = lax.fori_loop(
        0, STEPS, norm, (zero, zero, (zero,) * LANES, (zero,) * LANES)
    )
    stat_out[1, 0] = one
    stat_out[1, 1] = two
    for l in range(LANES):
        parts[l, 8 * KERNEL : 8 * KERNEL + 8] = by_gain[l]
        spare[8 * l : 8 * l + 8] = by_shift[l]
    one, two = of_pair(1)
    spread(one / width, first_b)
    spread(two / width, second_b)

    def folded(ref, start):
        rows = ref[pl.ds(start, 8, stride=8)]
        for s in range(1, SUB):
            rows = rows + ref[pl.ds(start + s, 8, stride=8)]
        return rows

    def to_axis(buffer, axis, here, count, index):
        def descriptor(step):
            _, device = along(axis, here, count, step)
            return exchange(
                buffer.at[here], buffer.at[here], sh_send.at[index], sh_recv.at[index], device
            )

        @pl.loop(1, count)
        def _(step):
            descriptor(step).start()

    def arrived(buffer, count, send, recv):
        if count > 1:
            some = buffer.at[pl.ds(0, count - 1)]
            pltpu.make_async_copy(some, some, recv).wait()
            pltpu.make_async_copy(some, some, send).wait()

    def from_axis(buffer, count, index):
        arrived(buffer, count, sh_send.at[index], sh_recv.at[index])
        result = buffer[0]
        for i in range(1, count):
            result = result + buffer[i]
        return result

    shift_x[x] = folded(spare, 0)
    to_axis(shift_x, "sp_2", x, nx, 0)

    @pl.loop(0, STEPS)
    def _(j):
        inv, one, two = inv_b[at_row(j)], first_b[at_row(j)], second_b[at_row(j)]
        for l in range(LANES):
            v = inv * (grad[l, at_row(j)] - one - conv[l, at_row(j)] * two)
            grad[l, at_row(j)] = v
            wide[l, pl.ds(PITCH + 16 + j, SUB, stride=PITCH)] = v
            wide[l, pl.ds(j + 48 + 80 * (j // 16), SUB, stride=PITCH)] = v

    for l in range(LANES):
        tail_out[0, l] = wide[l, 48:64]
        tail_out[1, l] = wide[l, 9 * PITCH : 9 * PITCH + 16]

    shift_y[y] = from_axis(shift_x, nx, 0)
    to_axis(shift_y, "sp_1", y, ny, 1)
    tails = [
        exchange(tail_out.at[0], tail_in.at[1], tail_send.at[0], tail_recv.at[1], before),
        exchange(tail_out.at[1], tail_in.at[0], tail_send.at[1], tail_recv.at[0], after),
    ]
    for copy in tails:
        copy.start()

    @pl.loop(0, LANES)
    def _(l):
        for k0 in range(0, KERNEL, GROUP):
            count = min(GROUP, KERNEL - k0)
            sums = [zero] * count
            window = [
                gated[l, pl.ds(PITCH + 1 + k0 + i, SUB, stride=PITCH)]
                for i in range(STEPS + count - 1)
            ]
            for j in range(STEPS):
                g = grad[l, pl.ds(8 * j, 8)]
                for i in range(count):
                    sums[i] = sums[i] + g * window[j + i]
            for i in range(count):
                parts[l, pl.ds(8 * (k0 + i), 8)] = sums[i]
        for g in range(4):
            tiles[g * LANES + l] = folded(parts.at[l], 64 * g)

    shift_z[z] = from_axis(shift_y, ny, 1)

    @pl.loop(1, plane)
    def _(step):
        q, device = in_plane(step)
        exchange(tiles.at[q], tiles_in.at[mine], rs_send, rs_recv, device).start()

    to_axis(shift_z, "sp_0", z, nz, 2)

    for copy in tails:
        copy.wait()
    for i, start in enumerate((PITCH, SUB * PITCH + 48)):
        for l in range(LANES):
            wide[l, pl.ds(start, 16)] = jnp.where(absent[i], 0.0, tail_in[i, l])

    @pl.loop(0, LANES)
    def _(l):
        for j0 in range(0, STEPS, GROUP):
            low = PITCH + 31 - (KERNEL - 1) + j0
            window = [
                wide[l, pl.ds(low + i, SUB, stride=PITCH)] for i in range(GROUP + KERNEL - 1)
            ]
            sums = [zero] * GROUP
            for k in range(KERNEL):
                weight = tap(k, l)
                for i in range(GROUP):
                    sums[i] = sums[i] + weight * window[i + KERNEL - 1 - k]
            for i in range(GROUP):
                back[l, pl.ds(j0 + i, SUB, stride=OUT_PITCH)] = sums[i]

    @pl.loop(0, SUB)
    def _(s):
        for half in range(2):
            rows = pl.ds(pl.multiple_of(32 * s + 16 * half, 16), 16)
            for l in range(LANES):
                lanes = slice(128 * l, 128 * l + 128)
                g = back[l, pl.ds(pl.multiple_of(OUT_PITCH * s + 16 * half, 8), 16)]
                sig = sigmoid(gate[rows, lanes].astype(F32))
                d_value[rows, lanes] = (g * sig).astype(BF16)
                d_gate[rows, lanes] = (
                    g * value[rows, lanes].astype(F32) * sig * (1.0 - sig)
                ).astype(BF16)

    outs = [
        pltpu.make_async_copy(src, dst, out_sem.at[i])
        for i, (src, dst) in enumerate(
            [(d_value, d_value_hbm), (d_gate, d_gate_hbm), (d_taps, d_taps_hbm),
             (d_gain, d_gain_hbm), (d_shift, d_shift_hbm)]
        )
    ]
    outs[0].start()
    outs[1].start()

    scale = 1.0 / math.sqrt(total)
    arrived(tiles_in, plane, rs_send, rs_recv)
    line_own = tiles[mine]
    tiles_in[mine] = line_own
    halves = [tiles_in[0], tiles_in[1]]
    for i in range(2, plane):
        halves[i % 2] = halves[i % 2] + tiles_in[i]
    line[z] = halves[0] + halves[1]

    @pl.loop(1, nz)
    def _(step):
        _, device = along("sp_0", z, nz, step)
        exchange(line.at[z], line.at[z], z_send, z_recv, device).start()

    d_shift[...] = from_axis(shift_z, nz, 2) * scale
    outs[4].start()

    arrived(line, nz, z_send, z_recv)
    result = line[0]
    for i in range(1, nz):
        result = result + line[i]
    final[mine] = result * scale

    @pl.loop(1, plane)
    def _(step):
        _, device = in_plane(step)
        exchange(final.at[mine], final.at[mine], ag_send, ag_recv, device).start()

    arrived(final, plane, ag_send, ag_recv)
    for g in range(4):
        for l in range(LANES):
            lanes = slice(128 * l, 128 * l + 128)
            if g < 3:
                d_taps[8 * g : 8 * g + 8, lanes] = final[g * LANES + l]
            else:
                last = final[g * LANES + l]
                d_taps[24:KERNEL, lanes] = last[:7]
                d_gain[:, lanes] = last[7:]
    outs[2].start()
    outs[3].start()
    for copy in outs:
        copy.wait()


def shards(dims, total, value_in, gate_in, taps, gain, shift, w_out, grad_out):
    nz, ny, nx = dims
    depth = grad_out.shape[1]
    vmem = pltpu.VMEM
    dma = pltpu.SemaphoreType.DMA
    padded = (LANES, 10 * PITCH, 128)
    rows = (LANES, ROWS, 128)
    spread = (LANES, SUB * OUT_PITCH, 128)
    scratch = [
        vmem((ROWS, WIDTH), BF16), vmem((ROWS, WIDTH), BF16), vmem((KERNEL, WIDTH), F32),
        vmem((1, WIDTH), F32), vmem((1, WIDTH), F32), vmem((WIDTH, depth), BF16),
        vmem((ROWS, depth), BF16),
        vmem(padded, F32), vmem(rows, F32), vmem(spread, F32), vmem(rows, F32),
        vmem(padded, F32), vmem(spread, F32), vmem(rows, F32), vmem((8, 128), F32),
        vmem((2, 16, WIDTH), BF16), vmem((2, 16, WIDTH), BF16),
        vmem((2, LANES, 16, 128), F32), vmem((2, LANES, 16, 128), F32),
        vmem((2, 2, SUB, 128), F32), vmem((2, 2, SUB, 128), F32),
        vmem((ROWS, 128), F32), vmem((ROWS, 128), F32), vmem((ROWS, 128), F32),
        vmem((ROWS, 128), F32),
        vmem((32, 8, 128), F32), vmem((32, 8, 128), F32), vmem((nz, 8, 128), F32),
        vmem((32, 8, 128), F32), vmem((nx, 8, 128), F32), vmem((ny, 8, 128), F32),
        vmem((nz, 8, 128), F32), vmem((64, 128), F32),
        vmem((ROWS, WIDTH), BF16), vmem((ROWS, WIDTH), BF16), vmem((KERNEL, WIDTH), F32),
        vmem((1, WIDTH), F32), vmem((8, 128), F32),
        dma((6,)), dma((4,)), dma((2,)), dma((2,)), dma((2,)), dma((2,)), dma((2,)), dma((2,)),
        dma, dma, dma, dma, dma, dma, dma((3,)), dma((3,)), dma((5,)),
    ]
    anywhere = pl.BlockSpec(memory_space=pl.ANY)
    shape = jax.ShapeDtypeStruct
    d_value, d_gate, d_taps, d_gain, d_shift = pl.pallas_call(
        functools.partial(kernel, dims, total),
        out_shape=(
            shape((ROWS, WIDTH), BF16), shape((ROWS, WIDTH), BF16), shape((KERNEL, WIDTH), F32),
            shape((1, WIDTH), F32), shape((8, 128), F32),
        ),
        in_specs=[anywhere] * 7,
        out_specs=(anywhere,) * 5,
        scratch_shapes=scratch,
        compiler_params=pltpu.CompilerParams(
            collective_id=0, has_side_effects=True, vmem_limit_bytes=48 * 2**20
        ),
        name="module",
    )(value_in, gate_in, taps, gain.reshape(1, WIDTH), shift.reshape(1, WIDTH), w_out, grad_out)
    return d_value, d_gate, d_taps, d_gain.reshape(WIDTH), d_shift.reshape(WIDTH)


def solution(mesh, dims=(12, 8, 4)):
    finer = Mesh(mesh.devices.reshape(*dims, mesh.shape["tp"]), (*SP, "tp"))
    total = ROWS * math.prod(dims)
    return jax.shard_map(
        functools.partial(shards, dims, total),
        mesh=finer,
        in_specs=(
            P(SP, "tp"), P(SP, "tp"), P(None, "tp"), P("tp"), P("tp"), P("tp", None), P(SP, None),
        ),
        out_specs=(P(SP, "tp"), P(SP, "tp"), P(None, "tp"), P("tp"), P("tp")),
        check_vma=False,
    )
```

```python
import functools
import math

import jax
import jax.numpy as jnp
from jax import lax
from jax.experimental import pallas as pl
from jax.experimental.pallas import tpu as pltpu
from jax.sharding import Mesh
from jax.sharding import PartitionSpec as P

SP = ("sp_0", "sp_1", "sp_2")
EPS = 1e-05
F32 = jnp.float32
BF16 = jnp.bfloat16
MESH = pl.DeviceIdType.MESH

ROWS, WIDTH, KERNEL, HALF = 256, 1024, 31, 15
LANES, SUB, STEPS, PITCH, OUT_PITCH = 8, 8, 32, 72, 40
GROUP = 8


def position(dims):
    nz, ny, nx = dims
    z, y, x = (lax.axis_index(a) for a in SP)
    return z, y, x, lax.axis_index("tp"), (z * ny + y) * nx + x


def place(index, dims):
    nz, ny, nx = dims
    return {"sp_0": index // (ny * nx), "sp_1": (index // nx) % ny, "sp_2": index % nx}


def sigmoid(v):
    return jax.nn.sigmoid(v)


class Phases:
    def __init__(self):
        self.open = None

    def __call__(self, name):
        if self.open is not None:
            self.open.__exit__(None, None, None)
        self.open = None if name is None else jax.named_scope(name)
        if self.open is not None:
            self.open.__enter__()


def kernel(
    dims,
    total,
    value_hbm, gate_hbm, taps_hbm, gain_hbm, shift_hbm, w_hbm, cot_hbm,
    d_value, d_gate, d_taps, d_gain, d_shift,
    value, gate, taps, gain, shift, w, cot,
    gated, conv, mix, grad, wide, back, parts, bits,
    edge_out, edge_in, edge, tail_out, tail_in,
    stat_out, stat_in, mean_b, inv_b, first_b, second_b,
    tiles, tiles_in, line, final, shift_x, shift_y, shift_z, spare,
    in_sem, w_sem, edge_send, edge_recv, stat_send, stat_recv, tail_send, tail_recv,
    rs_send, rs_recv, z_send, z_recv, ag_send, ag_recv, sh_send, sh_recv,
):
    nz, ny, nx = dims
    z, y, x, t, me = position(dims)
    n_sp = nz * ny * nx
    plane = ny * nx
    mine = x * ny + y
    after = place(lax.rem(me + 1, n_sp), dims)
    before = place(lax.rem(me + n_sp - 1, n_sp), dims)
    partner = {"tp": 1 - t}

    def far_first(count):
        return sorted(range(1, count), key=lambda step: -min(step, count - step))

    def ring(here, count):
        return [here] + [lax.rem(here + step, count) for step in range(1, count)]

    xs, ys, zs = ring(x, nx), ring(y, ny), ring(z, nz)
    in_plane = [
        {"sp_1": ys[dy], "sp_2": xs[dx]}
        for dx, dy in sorted(
            [(dx, dy) for dx in range(nx) for dy in range(ny) if dx or dy],
            key=lambda d: -(min(d[0], nx - d[0]) + min(d[1], ny - d[1])),
        )
    ]

    def along(axis, places):
        return [{axis: places[step]} for step in far_first(len(places))]

    phase = Phases()

    small = [
        pltpu.make_async_copy(src, dst, in_sem.at[i])
        for i, (src, dst) in enumerate(
            [(value_hbm, value), (gate_hbm, gate), (taps_hbm, taps), (gain_hbm, gain),
             (shift_hbm, shift), (cot_hbm, cot)]
        )
    ]
    big = [
        pltpu.make_async_copy(
            w_hbm.at[pl.ds(256 * i, 256)], w.at[pl.ds(256 * i, 256)], w_sem.at[i]
        )
        for i in range(4)
    ]
    small[0].start()
    small[1].start()
    small[5].start()
    for copy in big:
        copy.start()
    for i in (2, 3, 4):
        small[i].start()

    phase("greet")
    barrier = pltpu.get_barrier_semaphore()

    def greet(device):
        pl.semaphore_signal(barrier, inc=1, device_id=device, device_id_type=MESH)

    for device in along("sp_0", zs) + in_plane + [after, before, partner]:
        greet(device)

    phase("load")
    small[0].wait()
    small[1].wait()

    def gated_of(rows, lanes):
        sig = sigmoid(gate[rows, lanes].astype(F32))
        return (value[rows, lanes].astype(F32) * sig).astype(BF16)

    phase("gate")
    for i, start in enumerate((0, ROWS - 16)):
        edge_out[i] = gated_of(pl.ds(start, 16), slice(None))

    starts = (PITCH, SUB * PITCH + 48)
    for l in range(LANES):
        for start in starts:
            gated[l, pl.ds(start, 16)] = jnp.zeros((16, 128), F32)
        edge[l, 16:32] = jnp.zeros((16, 128), F32)

    @pl.loop(0, SUB)
    def _(s):
        for half in range(2):
            rows = pl.ds(pl.multiple_of(32 * s + 16 * half, 16), 16)
            for l in range(LANES):
                v = gated_of(rows, slice(128 * l, 128 * l + 128)).astype(F32)
                own = pl.multiple_of(PITCH * (s + 1) + 16 + 16 * half, 8)
                gated[l, pl.ds(own, 16)] = v
                other = pl.multiple_of(PITCH * s + 48 if half == 0 else PITCH * (s + 2), 8)
                gated[l, pl.ds(other, 16)] = v

    phase("project")
    small[5].wait()
    for i in range(4):
        big[i].wait()
        product = lax.dot_general(
            cot[...], w[pl.ds(256 * i, 256)], (((1,), (1,)), ((), ())),
            preferred_element_type=F32,
        )
        for part in range(2):
            for s in range(SUB):
                mix[2 * i + part, pl.ds(OUT_PITCH * s, 32)] = product[
                    32 * s : 32 * s + 32, 128 * part : 128 * part + 128
                ]

    for i in (2, 3, 4):
        small[i].wait()

    phase("barrier")
    pl.semaphore_wait(barrier, (nz - 1) + (plane - 1) + 3)

    def exchange(source, target, send, recv, device):
        return pltpu.make_async_remote_copy(
            src_ref=source, dst_ref=target, send_sem=send, recv_sem=recv,
            device_id=device, device_id_type=MESH,
        )

    phase("edges")
    edges = [
        exchange(edge_out.at[0], edge_in.at[1], edge_send.at[0], edge_recv.at[1], before),
        exchange(edge_out.at[1], edge_in.at[0], edge_send.at[1], edge_recv.at[0], after),
    ]
    for copy in edges:
        copy.start()
    def tap(k, l):
        lanes = pl.ds(pl.multiple_of(128 * l, 128), 128)
        return jnp.broadcast_to(taps[pl.ds(k, 1), lanes], (SUB, 128))

    phase("conv")
    @pl.loop(0, LANES)
    def _(l):
        for j0 in range(0, STEPS, GROUP):
            window = [
                gated[l, pl.ds(PITCH + j0 + 1 + i, SUB, stride=PITCH)]
                for i in range(GROUP + KERNEL - 1)
            ]
            sums = [jnp.zeros((SUB, 128), F32)] * GROUP
            for k in range(KERNEL):
                weight = tap(k, l)
                for i in range(GROUP):
                    sums[i] = sums[i] + weight * window[i + k]
            for i in range(GROUP):
                conv[l, pl.ds(8 * (j0 + i), 8)] = sums[i]

    phase("edges_wait")
    for copy in edges:
        copy.wait()
    phase("fill")
    absent = (me == 0, me == n_sp - 1)
    for i in range(2):
        for l in range(LANES):
            v = edge_in[i, :, 128 * l : 128 * l + 128].astype(F32)
            v = jnp.where(absent[i], 0.0, v)
            gated[l, pl.ds(starts[i], 16)] = v
            edge[l, pl.ds(32 * i, 16)] = v

    @pl.loop(0, LANES)
    def _(l):
        for t0 in (0, 8):
            low = jnp.zeros((SUB, 128), F32)
            for k in range(HALF - t0):
                low = low + tap(k, l) * edge[l, pl.ds(t0 + k + 1, 8)]
            rows = pl.ds(8 * t0, 8, stride=8)
            conv[l, rows] = conv[l, rows] + low
            high = jnp.zeros((SUB, 128), F32)
            for k in range(24 - t0, KERNEL):
                high = high + tap(k, l) * edge[l, pl.ds(t0 + k + 1, 8)]
            rows = pl.ds(8 * (16 + t0) + 7, 8, stride=8)
            conv[l, rows] = conv[l, rows] + high

    lane = lax.broadcasted_iota(jnp.int32, (SUB, 128), 1)
    zero = jnp.zeros((SUB, 128), F32)

    def at_row(j):
        return pl.ds(pl.multiple_of(8 * j, 8), 8)

    def packed(ref):
        result = zero
        for j in range(STEPS):
            row = jnp.sum(ref[8 * j : 8 * j + 8], 1, keepdims=True)
            result = jnp.where(lane == j, row, result)
        return result

    def of_pair(slot):
        copy = exchange(
            stat_out.at[slot], stat_in.at[slot], stat_send.at[slot], stat_recv.at[slot], partner
        )
        copy.start()
        copy.wait()
        return (
            stat_out[slot, 0] + stat_in[slot, 0],
            stat_out[slot, 1] + stat_in[slot, 1],
        )

    def spread(stat, target):
        for j in range(STEPS):
            target[8 * j : 8 * j + 8] = jnp.broadcast_to(stat[:, j : j + 1], (SUB, 128))

    phase("totals")

    @pl.loop(0, STEPS, unroll=4)
    def _(j):
        one, two = zero, zero
        for l in range(LANES):
            v = conv[l, at_row(j)]
            one = one + v
            two = two + v * v
        first_b[at_row(j)] = one
        second_b[at_row(j)] = two

    stat_out[0, 0] = packed(first_b)
    stat_out[0, 1] = packed(second_b)
    phase("pair0")
    one, two = of_pair(0)
    phase("spread0")
    width = 2.0 * WIDTH
    mean = one / width
    inv = lax.rsqrt(two / width - mean * mean + EPS)
    spread(mean, mean_b)
    spread(inv, inv_b)

    def norm(j, carry):
        by_gain, by_shift = (list(part) for part in carry)
        mean, inv = mean_b[at_row(j)], inv_b[at_row(j)]
        one, two = zero, zero
        for l in range(LANES):
            lanes = slice(128 * l, 128 * l + 128)
            g = gain[:, lanes]
            normed = (conv[l, at_row(j)] - mean) * inv
            pre = normed * g + shift[:, lanes]
            sig = sigmoid(pre)
            grad_pre = mix[l, pl.ds(j, SUB, stride=OUT_PITCH)] * sig * (1.0 + pre * (1.0 - sig))
            grad_normed = grad_pre * g
            one = one + grad_normed
            two = two + grad_normed * normed
            by_gain[l] = by_gain[l] + grad_pre * normed
            by_shift[l] = by_shift[l] + grad_pre
            conv[l, at_row(j)] = normed
            grad[l, at_row(j)] = grad_normed
        first_b[at_row(j)] = one
        second_b[at_row(j)] = two
        return tuple(by_gain), tuple(by_shift)

    phase("norm")
    by_gain, by_shift = lax.fori_loop(
        0, STEPS, norm, ((zero,) * LANES, (zero,) * LANES)
    )
    stat_out[1, 0] = packed(first_b)
    stat_out[1, 1] = packed(second_b)
    for l in range(LANES):
        parts[l, 8 * KERNEL : 8 * KERNEL + 8] = by_gain[l]
        spare[8 * l : 8 * l + 8] = by_shift[l]
    phase("pair1")
    one, two = of_pair(1)
    phase("spread1")
    spread(one / width, first_b)
    spread(two / width, second_b)

    def folded(ref, start):
        rows = ref[pl.ds(start, 8, stride=8)]
        for s in range(1, SUB):
            rows = rows + ref[pl.ds(start + s, 8, stride=8)]
        return rows

    def to_axis(buffer, axis, places, index):
        own = buffer.at[places[0]]
        for device in along(axis, places):
            exchange(own, own, sh_send.at[index], sh_recv.at[index], device).start()

    def arrived(buffer, count, send, recv):
        if count > 1:
            some = buffer.at[pl.ds(0, count - 1)]
            pltpu.make_async_copy(some, some, recv).wait()
            pltpu.make_async_copy(some, some, send).wait()

    def from_axis(buffer, count, index):
        arrived(buffer, count, sh_send.at[index], sh_recv.at[index])
        result = buffer[0]
        for i in range(1, count):
            result = result + buffer[i]
        return result

    phase("gradconv")
    shift_x[x] = folded(spare, 0)
    to_axis(shift_x, "sp_2", xs, 0)

    @pl.loop(0, STEPS)
    def _(j):
        inv, one, two = inv_b[at_row(j)], first_b[at_row(j)], second_b[at_row(j)]
        for l in range(LANES):
            v = inv * (grad[l, at_row(j)] - one - conv[l, at_row(j)] * two)
            grad[l, at_row(j)] = v
            wide[l, pl.ds(PITCH + 16 + j, SUB, stride=PITCH)] = v
            wide[l, pl.ds(j + 48 + 80 * (j // 16), SUB, stride=PITCH)] = v

    for l in range(LANES):
        tail_out[0, l] = wide[l, 48:64]
        tail_out[1, l] = wide[l, 9 * PITCH : 9 * PITCH + 16]

    tails = [
        exchange(tail_out.at[0], tail_in.at[1], tail_send.at[0], tail_recv.at[1], before),
        exchange(tail_out.at[1], tail_in.at[0], tail_send.at[1], tail_recv.at[0], after),
    ]
    for copy in tails:
        copy.start()

    def send_tile(g, l, device_x, device_y):
        q = g * LANES + l
        exchange(
            tiles.at[q], tiles_in.at[mine], rs_send, rs_recv, {"sp_1": device_y, "sp_2": device_x}
        ).start()

    def lane_block(i):
        odd = lax.rem(i, 2)
        offset = LANES // 2 + (i // 2) * (1 - odd) - ((i + 1) // 2) * odd
        return lax.rem(y + offset, LANES)

    phase("taps")

    @pl.loop(0, LANES)
    def _(i):
        l = lane_block(i)
        for k0 in range(0, KERNEL, GROUP):
            count = min(GROUP, KERNEL - k0)
            sums = [zero] * count
            window = [
                gated[l, pl.ds(PITCH + 1 + k0 + n, SUB, stride=PITCH)]
                for n in range(STEPS + count - 1)
            ]
            for j in range(STEPS):
                g = grad[l, pl.ds(8 * j, 8)]
                for n in range(count):
                    sums[n] = sums[n] + g * window[j + n]
            for n in range(count):
                parts[l, pl.ds(8 * (k0 + n), 8)] = sums[n]
        for g in range(4):
            tiles[g * LANES + l] = folded(parts.at[l], 64 * g)

        @pl.when(i > 0)
        def _():
            done = lane_block(i - 1)
            for step in (2, 1, 3, 0):
                send_tile(xs[step], done, xs[step], done)

    phase("rs_start")
    for step in far_first(nx):
        send_tile(xs[step], y, xs[step], y)
    shift_y[y] = from_axis(shift_x, nx, 0)
    to_axis(shift_y, "sp_1", ys, 1)

    phase("tails")
    for copy in tails:
        copy.wait()
    for i in range(2):
        for l in range(LANES):
            wide[l, pl.ds(starts[i], 16)] = jnp.where(absent[i], 0.0, tail_in[i, l])

    phase("back")
    @pl.loop(0, LANES)
    def _(l):
        for j0 in range(0, STEPS, GROUP):
            low = PITCH + 31 - (KERNEL - 1) + j0
            window = [
                wide[l, pl.ds(low + i, SUB, stride=PITCH)] for i in range(GROUP + KERNEL - 1)
            ]
            sums = [zero] * GROUP
            for k in range(KERNEL):
                weight = tap(k, l)
                for i in range(GROUP):
                    sums[i] = sums[i] + weight * window[i + KERNEL - 1 - k]
            for i in range(GROUP):
                back[l, pl.ds(j0 + i, SUB, stride=OUT_PITCH)] = sums[i]

    @pl.loop(0, SUB)
    def _(s):
        for half in range(2):
            rows = pl.ds(pl.multiple_of(32 * s + 16 * half, 16), 16)
            for l in range(LANES):
                lanes = slice(128 * l, 128 * l + 128)
                g = back[l, pl.ds(pl.multiple_of(OUT_PITCH * s + 16 * half, 8), 16)]
                sig = sigmoid(gate[rows, lanes].astype(F32))
                d_value[rows, lanes] = (g * sig).astype(BF16)
                d_gate[rows, lanes] = (
                    g * value[rows, lanes].astype(F32) * sig * (1.0 - sig)
                ).astype(BF16)

    phase("rs_wait")
    scale = 1.0 / math.sqrt(total)
    arrived(tiles_in, plane, rs_send, rs_recv)
    line_own = tiles[mine]
    phase("rs_sum")
    tiles_in[mine] = line_own
    halves = [tiles_in[0], tiles_in[1]]
    for i in range(2, plane):
        halves[i % 2] = halves[i % 2] + tiles_in[i]
    line[z] = halves[0] + halves[1]

    for device in along("sp_0", zs):
        exchange(line.at[z], line.at[z], z_send, z_recv, device).start()
    shift_z[z] = from_axis(shift_y, ny, 1)
    to_axis(shift_z, "sp_0", zs, 2)


    phase("z_wait")
    arrived(line, nz, z_send, z_recv)
    phase("ag_start")
    result = line[0]
    for i in range(1, nz):
        result = result + line[i]
    final[mine] = result * scale

    for device in in_plane:
        exchange(final.at[mine], final.at[mine], ag_send, ag_recv, device).start()
    d_shift[...] = from_axis(shift_z, nz, 2) * scale

    phase("ag_wait")
    arrived(final, plane, ag_send, ag_recv)
    phase("finish")
    for g in range(4):
        for l in range(LANES):
            lanes = slice(128 * l, 128 * l + 128)
            if g < 3:
                d_taps[8 * g : 8 * g + 8, lanes] = final[g * LANES + l]
            else:
                last = final[g * LANES + l]
                d_taps[24:KERNEL, lanes] = last[:7]
                d_gain[:, lanes] = last[7:]
    phase(None)


def shards(dims, total, value_in, gate_in, taps, gain, shift, w_out, grad_out):
    nz, ny, nx = dims
    depth = grad_out.shape[1]
    vmem = pltpu.VMEM
    dma = pltpu.SemaphoreType.DMA
    padded = (LANES, 10 * PITCH, 128)
    rows = (LANES, ROWS, 128)
    spread = (LANES, SUB * OUT_PITCH, 128)
    scratch = [
        vmem((ROWS, WIDTH), BF16), vmem((ROWS, WIDTH), BF16), vmem((KERNEL, WIDTH), F32),
        vmem((1, WIDTH), F32), vmem((1, WIDTH), F32), vmem((WIDTH, depth), BF16),
        vmem((ROWS, depth), BF16),
        vmem(padded, F32), vmem(rows, F32), vmem(spread, F32), vmem(rows, F32),
        vmem(padded, F32), vmem(spread, F32), vmem(rows, F32), vmem((8, 128), F32),
        vmem((2, 16, WIDTH), BF16), vmem((2, 16, WIDTH), BF16), vmem((LANES, 48, 128), F32),
        vmem((2, LANES, 16, 128), F32), vmem((2, LANES, 16, 128), F32),
        vmem((2, 2, SUB, 128), F32), vmem((2, 2, SUB, 128), F32),
        vmem((ROWS, 128), F32), vmem((ROWS, 128), F32), vmem((ROWS, 128), F32),
        vmem((ROWS, 128), F32),
        vmem((32, 8, 128), F32), vmem((32, 8, 128), F32), vmem((nz, 8, 128), F32),
        vmem((32, 8, 128), F32), vmem((nx, 8, 128), F32), vmem((ny, 8, 128), F32),
        vmem((nz, 8, 128), F32), vmem((64, 128), F32),
        dma((6,)), dma((4,)), dma((2,)), dma((2,)), dma((2,)), dma((2,)), dma((2,)), dma((2,)),
        dma, dma, dma, dma, dma, dma, dma((3,)), dma((3,)),
    ]
    hbm = pl.BlockSpec(memory_space=pltpu.HBM)
    near = pl.BlockSpec(memory_space=pltpu.VMEM)
    shape = jax.ShapeDtypeStruct
    shapes = (
        shape((ROWS, WIDTH), BF16), shape((ROWS, WIDTH), BF16), shape((KERNEL, WIDTH), F32),
        shape((1, WIDTH), F32), shape((8, 128), F32),
    )
    results = pl.pallas_call(
        functools.partial(kernel, dims, total),
        out_shape=shapes,
        in_specs=[hbm] * 7,
        out_specs=(near,) * 5,
        scratch_shapes=scratch,
        compiler_params=pltpu.CompilerParams(
            collective_id=0, has_side_effects=True, vmem_limit_bytes=40 * 2**20
        ),
        name="module",
    )(*(pltpu.with_memory_space_constraint(a, pltpu.HBM) for a in (value_in, gate_in, taps, gain.reshape(1, WIDTH), shift.reshape(1, WIDTH), w_out, grad_out)))
    d_value, d_gate, d_taps, d_gain, d_shift = pl.pallas_call(
        put_out,
        out_shape=shapes,
        in_specs=[pl.BlockSpec(memory_space=pl.ANY)] * 5,
        out_specs=(hbm,) * 5,
        scratch_shapes=[dma((5,))],
        compiler_params=pltpu.CompilerParams(vmem_limit_bytes=2**20),
        name="put_out",
    )(*results)
    return d_value, d_gate, d_taps, d_gain.reshape(WIDTH), d_shift.reshape(WIDTH)


def put_out(*refs):
    sems = refs[10]
    copies = [pltpu.make_async_copy(refs[i], refs[5 + i], sems.at[i]) for i in range(5)]
    for copy in copies:
        copy.start()
    for copy in copies:
        copy.wait()


def solution(mesh, dims=(12, 8, 4)):
    finer = Mesh(mesh.devices.reshape(*dims, mesh.shape["tp"]), (*SP, "tp"))
    total = ROWS * math.prod(dims)
    return jax.shard_map(
        functools.partial(shards, dims, total),
        mesh=finer,
        in_specs=(
            P(SP, "tp"), P(SP, "tp"), P(None, "tp"), P("tp"), P("tp"), P("tp", None), P(SP, None),
        ),
        out_specs=(P(SP, "tp"), P(SP, "tp"), P(None, "tp"), P("tp"), P("tp")),
        check_vma=False,
    )
```

```python
import functools
import math

import jax
import jax.numpy as jnp
from jax import lax
from jax.experimental import pallas as pl
from jax.experimental.pallas import tpu as pltpu
from jax.sharding import Mesh
from jax.sharding import PartitionSpec as P

SP = ("sp_0", "sp_1", "sp_2")
EPS = 1e-05
F32 = jnp.float32
BF16 = jnp.bfloat16
MESH = pl.DeviceIdType.MESH

ROWS, WIDTH, KERNEL, HALF = 256, 1024, 31, 15
ADDER = 1
ROUNDS = 6
LANES, SUB, STEPS, PITCH, OUT_PITCH = 8, 8, 32, 72, 40
GROUP = 8


def position(dims):
    nz, ny, nx = dims
    z, y, x = (lax.axis_index(a) for a in SP)
    return z, y, x, lax.axis_index("tp"), (z * ny + y) * nx + x


def place(index, dims):
    nz, ny, nx = dims
    return {"sp_0": index // (ny * nx), "sp_1": (index // nx) % ny, "sp_2": index % nx}


def sigmoid(v):
    return jax.nn.sigmoid(v)


class Phases:
    def __init__(self):
        self.open = None

    def __call__(self, name):
        if self.open is not None:
            self.open.__exit__(None, None, None)
        self.open = None if name is None else jax.named_scope(name)
        if self.open is not None:
            self.open.__enter__()


def kernel(
    dims,
    total,
    value_hbm, gate_hbm, taps_hbm, gain_hbm, shift_hbm, w_hbm, cot_hbm,
    d_value, d_gate, d_taps, d_gain, d_shift,
    value, gate, taps, gain, shift, w, cot,
    gated, conv, mix, grad, wide, back, parts, bits,
    edge_out, edge_in, edge, tail_out, tail_in, tail,
    stat_out, stat_in, mean_b, inv_b, first_b, second_b,
    tiles, tiles_in, line, final, other, shift_x, shift_y, shift_z, spare,
    in_sem, w_sem, edge_send, edge_recv, stat_send, stat_recv, tail_send, tail_recv,
    rs_send, rs_recv, z_send, z_recv, ag_send, ag_recv, sh_send, sh_recv, rounds,
):
    nz, ny, nx = dims
    z, y, x, t, me = position(dims)
    n_sp = nz * ny * nx
    plane = ny * nx
    mine = x * ny + y
    after = place(lax.rem(me + 1, n_sp), dims)
    before = place(lax.rem(me + n_sp - 1, n_sp), dims)
    partner = {"tp": 1 - t}

    def far_first(count):
        return sorted(range(1, count), key=lambda step: -min(step, count - step))

    def ring(here, count):
        return [here] + [lax.rem(here + step, count) for step in range(1, count)]

    xs, ys, zs = ring(x, nx), ring(y, ny), ring(z, nz)
    in_plane = [
        {"sp_1": ys[dy], "sp_2": xs[dx]}
        for dx, dy in sorted(
            [(dx, dy) for dx in range(nx) for dy in range(ny) if dx or dy],
            key=lambda d: -(min(d[0], nx - d[0]) + min(d[1], ny - d[1])),
        )
    ]

    def along(axis, places):
        return [{axis: places[step]} for step in far_first(len(places))]

    phase = Phases()

    small = [
        pltpu.make_async_copy(src, dst, in_sem.at[i])
        for i, (src, dst) in enumerate(
            [(value_hbm, value), (gate_hbm, gate), (taps_hbm, taps), (gain_hbm, gain),
             (shift_hbm, shift), (cot_hbm, cot)]
        )
    ]
    big = [
        pltpu.make_async_copy(
            w_hbm.at[pl.ds(256 * i, 256)], w.at[pl.ds(256 * i, 256)], w_sem.at[i]
        )
        for i in range(4)
    ]
    for copy in small + big:
        copy.start()

    phase("greet")
    barrier = pltpu.get_barrier_semaphore()

    def greet(device):
        pl.semaphore_signal(barrier, inc=1, device_id=device, device_id_type=MESH)

    def core(device, which):
        return {**device, "tp": which}

    beside = [
        {axis: places[step]}
        for axis, places in (("sp_2", xs), ("sp_1", ys), ("sp_0", zs))
        for step in (1, -1)
        if len(places) > 1
    ]
    for device in [after, before, partner] + beside:
        greet(device)

    def tell(turn):
        for device in beside:
            pl.semaphore_signal(
                rounds.at[turn], inc=1, device_id=device, device_id_type=MESH
            )

    def hear(turn):
        pl.semaphore_wait(rounds.at[turn], len(beside))
        if turn + 1 < ROUNDS:
            tell(turn + 1)

    phase("load")
    small[0].wait()
    small[1].wait()

    def gated_of(rows, lanes):
        sig = sigmoid(gate[rows, lanes].astype(F32))
        return (value[rows, lanes].astype(F32) * sig).astype(BF16)

    phase("gate")
    for i, start in enumerate((0, ROWS - 16)):
        edge_out[i] = gated_of(pl.ds(start, 16), slice(None))

    starts = (PITCH, SUB * PITCH + 48)
    for l in range(LANES):
        for start in starts:
            gated[l, pl.ds(start, 16)] = jnp.zeros((16, 128), F32)
            wide[l, pl.ds(start, 16)] = jnp.zeros((16, 128), F32)
        edge[l, 16:32] = jnp.zeros((16, 128), F32)
        tail[l, 16:32] = jnp.zeros((16, 128), F32)

    @pl.loop(0, SUB)
    def _(s):
        for half in range(2):
            rows = pl.ds(pl.multiple_of(32 * s + 16 * half, 16), 16)
            for l in range(LANES):
                v = gated_of(rows, slice(128 * l, 128 * l + 128)).astype(F32)
                own = pl.multiple_of(PITCH * (s + 1) + 16 + 16 * half, 8)
                gated[l, pl.ds(own, 16)] = v
                other = pl.multiple_of(PITCH * s + 48 if half == 0 else PITCH * (s + 2), 8)
                gated[l, pl.ds(other, 16)] = v

    for i in (2, 3, 4):
        small[i].wait()

    def tap(k, l):
        lanes = pl.ds(pl.multiple_of(128 * l, 128), 128)
        return jnp.broadcast_to(taps[pl.ds(k, 1), lanes], (SUB, 128))

    def project(i):
        big[i].wait()
        product = lax.dot_general(
            cot[...], w[pl.ds(256 * i, 256)], (((1,), (1,)), ((), ())),
            preferred_element_type=F32,
        )
        for part in range(2):
            for s in range(SUB):
                mix[2 * i + part, pl.ds(OUT_PITCH * s, 32)] = product[
                    32 * s : 32 * s + 32, 128 * part : 128 * part + 128
                ]

    phase("conv")
    def convolve(l):
        for j0 in range(0, STEPS, GROUP):
            window = [
                gated[l, pl.ds(PITCH + j0 + 1 + i, SUB, stride=PITCH)]
                for i in range(GROUP + KERNEL - 1)
            ]
            sums = [jnp.zeros((SUB, 128), F32)] * GROUP
            for k in range(KERNEL):
                weight = tap(k, l)
                for i in range(GROUP):
                    sums[i] = sums[i] + weight * window[i + k]
            for i in range(GROUP):
                conv[l, pl.ds(8 * (j0 + i), 8)] = sums[i]

    pl.loop(0, LANES // 2)(convolve)

    phase("barrier")
    pl.semaphore_wait(barrier, 3 + len(beside))
    tell(0)

    def exchange(source, target, send, recv, device):
        return pltpu.make_async_remote_copy(
            src_ref=source, dst_ref=target, send_sem=send, recv_sem=recv,
            device_id=device, device_id_type=MESH,
        )

    phase("edges")
    edges = [
        exchange(edge_out.at[0], edge_in.at[1], edge_send.at[0], edge_recv.at[1], before),
        exchange(edge_out.at[1], edge_in.at[0], edge_send.at[1], edge_recv.at[0], after),
    ]
    for copy in edges:
        copy.start()
    phase("conv2")
    pl.loop(LANES // 2, LANES)(convolve)
    hear(0)

    phase("project")
    small[5].wait()
    project(0)
    project(1)
    hear(1)
    project(2)
    hear(2)

    phase("edges_wait")
    for copy in edges:
        copy.wait()
    phase("fill")
    absent = (me == 0, me == n_sp - 1)
    for i in range(2):
        for l in range(LANES):
            v = edge_in[i, :, 128 * l : 128 * l + 128].astype(F32)
            v = jnp.where(absent[i], 0.0, v)
            gated[l, pl.ds(starts[i], 16)] = v
            edge[l, pl.ds(32 * i, 16)] = v

    @pl.loop(0, LANES)
    def _(l):
        for t0 in (0, 8):
            low = jnp.zeros((SUB, 128), F32)
            for k in range(HALF - t0):
                low = low + tap(k, l) * edge[l, pl.ds(t0 + k + 1, 8)]
            rows = pl.ds(8 * t0, 8, stride=8)
            conv[l, rows] = conv[l, rows] + low
            high = jnp.zeros((SUB, 128), F32)
            for k in range(24 - t0, KERNEL):
                high = high + tap(k, l) * edge[l, pl.ds(t0 + k + 1, 8)]
            rows = pl.ds(8 * (16 + t0) + 7, 8, stride=8)
            conv[l, rows] = conv[l, rows] + high

    lane = lax.broadcasted_iota(jnp.int32, (SUB, 128), 1)
    zero = jnp.zeros((SUB, 128), F32)

    def at_row(j):
        return pl.ds(pl.multiple_of(8 * j, 8), 8)

    def packed(ref):
        result = zero
        for j in range(STEPS):
            row = jnp.sum(ref[8 * j : 8 * j + 8], 1, keepdims=True)
            result = jnp.where(lane == j, row, result)
        return result

    def to_pair(slot):
        copy = exchange(
            stat_out.at[slot], stat_in.at[slot], stat_send.at[slot], stat_recv.at[slot], partner
        )
        copy.start()
        return copy

    def of_pair(copy, slot):
        copy.wait()
        return (
            stat_out[slot, 0] + stat_in[slot, 0],
            stat_out[slot, 1] + stat_in[slot, 1],
        )

    def spread(stat, target):
        for j in range(STEPS):
            target[8 * j : 8 * j + 8] = jnp.broadcast_to(stat[:, j : j + 1], (SUB, 128))

    phase("totals")

    @pl.loop(0, STEPS, unroll=4)
    def _(j):
        one, two = zero, zero
        for l in range(LANES):
            v = conv[l, at_row(j)]
            one = one + v
            two = two + v * v
        first_b[at_row(j)] = one
        second_b[at_row(j)] = two

    stat_out[0, 0] = packed(first_b)
    stat_out[0, 1] = packed(second_b)
    phase("pair0")
    copy = to_pair(0)
    hear(3)
    project(3)
    phase("pair0_wait")
    one, two = of_pair(copy, 0)
    phase("spread0")
    width = 2.0 * WIDTH
    mean = one / width
    inv = lax.rsqrt(two / width - mean * mean + EPS)
    spread(mean, mean_b)
    spread(inv, inv_b)

    def norm(j, carry):
        by_gain, by_shift = (list(part) for part in carry)
        mean, inv = mean_b[at_row(j)], inv_b[at_row(j)]
        one, two = zero, zero
        for l in range(LANES):
            lanes = slice(128 * l, 128 * l + 128)
            g = gain[:, lanes]
            normed = (conv[l, at_row(j)] - mean) * inv
            pre = normed * g + shift[:, lanes]
            sig = sigmoid(pre)
            grad_pre = mix[l, pl.ds(j, SUB, stride=OUT_PITCH)] * sig * (1.0 + pre * (1.0 - sig))
            grad_normed = grad_pre * g
            one = one + grad_normed
            two = two + grad_normed * normed
            by_gain[l] = by_gain[l] + grad_pre * normed
            by_shift[l] = by_shift[l] + grad_pre
            conv[l, at_row(j)] = normed
            grad[l, at_row(j)] = grad_normed
        first_b[at_row(j)] = one
        second_b[at_row(j)] = two
        return tuple(by_gain), tuple(by_shift)

    phase("norm")
    by_gain, by_shift = lax.fori_loop(
        0, STEPS, norm, ((zero,) * LANES, (zero,) * LANES)
    )
    stat_out[1, 0] = packed(first_b)
    stat_out[1, 1] = packed(second_b)
    phase("pair1")
    copy = to_pair(1)
    hear(4)
    for l in range(LANES):
        parts[l, 8 * KERNEL : 8 * KERNEL + 8] = by_gain[l]
        spare[8 * l : 8 * l + 8] = by_shift[l]
    one, two = of_pair(copy, 1)
    phase("spread1")
    spread(one / width, first_b)
    spread(two / width, second_b)

    def folded(ref, start):
        rows = ref[pl.ds(start, 8, stride=8)]
        for s in range(1, SUB):
            rows = rows + ref[pl.ds(start + s, 8, stride=8)]
        return rows

    def to_axis(buffer, axis, places, index):
        own = buffer.at[places[0]]
        for device in along(axis, places):
            exchange(own, own, sh_send.at[index], sh_recv.at[index], device).start()

    def arrived(buffer, count, send, recv):
        if count > 1:
            some = buffer.at[pl.ds(0, count - 1)]
            pltpu.make_async_copy(some, some, recv).wait()
            pltpu.make_async_copy(some, some, send).wait()

    def from_axis(buffer, count, index):
        arrived(buffer, count, sh_send.at[index], sh_recv.at[index])
        result = buffer[0]
        for i in range(1, count):
            result = result + buffer[i]
        return result

    phase("gradconv")
    shift_x[x] = folded(spare, 0)
    to_axis(shift_x, "sp_2", xs, 0)

    @pl.loop(0, STEPS)
    def _(j):
        inv, one, two = inv_b[at_row(j)], first_b[at_row(j)], second_b[at_row(j)]
        for l in range(LANES):
            v = inv * (grad[l, at_row(j)] - one - conv[l, at_row(j)] * two)
            grad[l, at_row(j)] = v
            wide[l, pl.ds(PITCH + 16 + j, SUB, stride=PITCH)] = v
            wide[l, pl.ds(j + 48 + 80 * (j // 16), SUB, stride=PITCH)] = v

    for l in range(LANES):
        tail_out[0, l] = wide[l, 48:64]
        tail_out[1, l] = wide[l, 9 * PITCH : 9 * PITCH + 16]

    tails = [
        exchange(tail_out.at[0], tail_in.at[1], tail_send.at[0], tail_recv.at[1], before),
        exchange(tail_out.at[1], tail_in.at[0], tail_send.at[1], tail_recv.at[0], after),
    ]
    for copy in tails:
        copy.start()

    def send_tile(g, l, device_x, device_y):
        q = g * LANES + l
        exchange(
            tiles.at[q], tiles_in.at[t * plane + mine], rs_send, rs_recv,
            {"sp_1": device_y, "sp_2": device_x, "tp": ADDER},
        ).start()

    def lane_block(i):
        odd = lax.rem(i, 2)
        offset = LANES // 2 + (i // 2) * (1 - odd) - ((i + 1) // 2) * odd
        return lax.rem(y + offset, LANES)

    hear(5)
    phase("taps")

    @pl.loop(0, LANES)
    def _(i):
        l = lane_block(i)
        for k0 in range(0, KERNEL, GROUP):
            count = min(GROUP, KERNEL - k0)
            sums = [zero] * count
            window = [
                gated[l, pl.ds(PITCH + 1 + k0 + n, SUB, stride=PITCH)]
                for n in range(STEPS + count - 1)
            ]
            for j in range(STEPS):
                g = grad[l, pl.ds(8 * j, 8)]
                for n in range(count):
                    sums[n] = sums[n] + g * window[j + n]
            for n in range(count):
                parts[l, pl.ds(8 * (k0 + n), 8)] = sums[n]
        for g in range(4):
            tiles[g * LANES + l] = folded(parts.at[l], 64 * g)

        @pl.when(i > 0)
        def _():
            done = lane_block(i - 1)
            for step in (2, 1, 3, 0):
                send_tile(xs[step], done, xs[step], done)

    phase("rs_start")
    for step in far_first(nx):
        send_tile(xs[step], y, xs[step], y)

    @pl.when(t != ADDER)
    def _():
        send_tile(x, y, x, y)

    shift_y[y] = from_axis(shift_x, nx, 0)
    to_axis(shift_y, "sp_1", ys, 1)

    phase("back")
    @pl.loop(0, LANES)
    def _(l):
        for j0 in range(0, STEPS, GROUP):
            low = PITCH + 31 - (KERNEL - 1) + j0
            window = [
                wide[l, pl.ds(low + i, SUB, stride=PITCH)] for i in range(GROUP + KERNEL - 1)
            ]
            sums = [zero] * GROUP
            for k in range(KERNEL):
                weight = tap(k, l)
                for i in range(GROUP):
                    sums[i] = sums[i] + weight * window[i + KERNEL - 1 - k]
            for i in range(GROUP):
                back[l, pl.ds(j0 + i, SUB, stride=OUT_PITCH)] = sums[i]

    def taken(sem, count):
        some = tiles_in.at[pl.ds(0, count)]
        pltpu.make_async_copy(some, some, sem).wait()

    phase("rs_wait")

    @pl.when(t == ADDER)
    def _():
        taken(rs_recv, 2 * plane - 1)
        tiles_in[ADDER * plane + mine] = tiles[mine]
        for which in range(2):
            halves = [tiles_in[which * plane], tiles_in[which * plane + 1]]
            for i in range(2, plane):
                halves[i % 2] = halves[i % 2] + tiles_in[which * plane + i]
            line[z, which] = halves[0] + halves[1]
        for device in along("sp_0", zs):
            exchange(line.at[z], line.at[z], z_send, z_recv, device).start()

    phase("shift_z")
    shift_z[z] = from_axis(shift_y, ny, 1)
    to_axis(shift_z, "sp_0", zs, 2)

    phase("tails")
    for copy in tails:
        copy.wait()
    for i in range(2):
        for l in range(LANES):
            tail[l, pl.ds(32 * i, 16)] = jnp.where(absent[i], 0.0, tail_in[i, l])

    @pl.loop(0, LANES)
    def _(l):
        for t0 in (0, 8):
            low = zero
            for k in range(16 + t0, KERNEL):
                low = low + tap(k, l) * tail[l, pl.ds(31 + t0 - k, 8)]
            rows = pl.ds(t0, 8)
            back[l, rows] = back[l, rows] + low
            high = zero
            for k in range(7 + t0):
                high = high + tap(k, l) * tail[l, pl.ds(31 + t0 - k, 8)]
            rows = pl.ds(OUT_PITCH * 7 + 16 + t0, 8)
            back[l, rows] = back[l, rows] + high

    phase("outputs")

    @pl.loop(0, SUB)
    def _(s):
        for half in range(2):
            rows = pl.ds(pl.multiple_of(32 * s + 16 * half, 16), 16)
            for l in range(LANES):
                lanes = slice(128 * l, 128 * l + 128)
                g = back[l, pl.ds(pl.multiple_of(OUT_PITCH * s + 16 * half, 8), 16)]
                sig = sigmoid(gate[rows, lanes].astype(F32))
                d_value[rows, lanes] = (g * sig).astype(BF16)
                d_gate[rows, lanes] = (
                    g * value[rows, lanes].astype(F32) * sig * (1.0 - sig)
                ).astype(BF16)

    phase("rs_wait")
    scale = 1.0 / math.sqrt(total)
    phase("z_wait")

    @pl.when(t == ADDER)
    def _():
        arrived(line, nz, z_send, z_recv)
        one, two = line[0, 0], line[0, 1]
        for i in range(1, nz):
            one, two = one + line[i, 0], two + line[i, 1]
        final[mine] = two * scale
        other[...] = one * scale
        for device in in_plane:
            exchange(other, final.at[mine], ag_send, ag_recv, core(device, 1 - ADDER)).start()
            exchange(
                final.at[mine], final.at[mine], ag_send, ag_recv, core(device, ADDER)
            ).start()
        exchange(other, final.at[mine], ag_send, ag_recv, partner).start()

    phase("shift_wait")
    d_shift[...] = from_axis(shift_z, nz, 2) * scale
    phase("ag_wait")

    @pl.when(t == ADDER)
    def _():
        taken(ag_recv, plane - 1)
        taken(ag_send, 2 * plane - 1)
        taken(rs_send, plane - 1)

    @pl.when(t != ADDER)
    def _():
        taken(ag_recv, plane)
        taken(rs_send, plane)

    phase("finish")
    for g in range(4):
        for l in range(LANES):
            lanes = slice(128 * l, 128 * l + 128)
            if g < 3:
                d_taps[8 * g : 8 * g + 8, lanes] = final[g * LANES + l]
            else:
                last = final[g * LANES + l]
                d_taps[24:KERNEL, lanes] = last[:7]
                d_gain[:, lanes] = last[7:]
    phase(None)


def shards(dims, total, value_in, gate_in, taps, gain, shift, w_out, grad_out):
    nz, ny, nx = dims
    depth = grad_out.shape[1]
    vmem = pltpu.VMEM
    dma = pltpu.SemaphoreType.DMA
    padded = (LANES, 10 * PITCH, 128)
    rows = (LANES, ROWS, 128)
    spread = (LANES, SUB * OUT_PITCH, 128)
    scratch = [
        vmem((ROWS, WIDTH), BF16), vmem((ROWS, WIDTH), BF16), vmem((KERNEL, WIDTH), F32),
        vmem((1, WIDTH), F32), vmem((1, WIDTH), F32), vmem((WIDTH, depth), BF16),
        vmem((ROWS, depth), BF16),
        vmem(padded, F32), vmem(rows, F32), vmem(spread, F32), vmem(rows, F32),
        vmem(padded, F32), vmem(spread, F32), vmem(rows, F32), vmem((8, 128), F32),
        vmem((2, 16, WIDTH), BF16), vmem((2, 16, WIDTH), BF16), vmem((LANES, 48, 128), F32),
        vmem((2, LANES, 16, 128), F32), vmem((2, LANES, 16, 128), F32),
        vmem((LANES, 48, 128), F32),
        vmem((2, 2, SUB, 128), F32), vmem((2, 2, SUB, 128), F32),
        vmem((ROWS, 128), F32), vmem((ROWS, 128), F32), vmem((ROWS, 128), F32),
        vmem((ROWS, 128), F32),
        vmem((32, 8, 128), F32), vmem((64, 8, 128), F32), vmem((nz, 2, 8, 128), F32),
        vmem((32, 8, 128), F32), vmem((8, 128), F32), vmem((nx, 8, 128), F32), vmem((ny, 8, 128), F32),
        vmem((nz, 8, 128), F32), vmem((64, 128), F32),
        dma((6,)), dma((4,)), dma((2,)), dma((2,)), dma((2,)), dma((2,)), dma((2,)), dma((2,)),
        dma, dma, dma, dma, dma, dma, dma((3,)), dma((3,)),
        pltpu.SemaphoreType.REGULAR((ROUNDS,)),
    ]
    hbm = pl.BlockSpec(memory_space=pltpu.HBM)
    near = pl.BlockSpec(memory_space=pltpu.VMEM)
    shape = jax.ShapeDtypeStruct
    shapes = (
        shape((ROWS, WIDTH), BF16), shape((ROWS, WIDTH), BF16), shape((KERNEL, WIDTH), F32),
        shape((1, WIDTH), F32), shape((8, 128), F32),
    )
    results = pl.pallas_call(
        functools.partial(kernel, dims, total),
        out_shape=shapes,
        in_specs=[hbm] * 7,
        out_specs=(near,) * 5,
        scratch_shapes=scratch,
        compiler_params=pltpu.CompilerParams(
            collective_id=0, has_side_effects=True, vmem_limit_bytes=40 * 2**20
        ),
        name="module",
    )(*(pltpu.with_memory_space_constraint(a, pltpu.HBM) for a in (value_in, gate_in, taps, gain.reshape(1, WIDTH), shift.reshape(1, WIDTH), w_out, grad_out)))
    d_value, d_gate, d_taps, d_gain, d_shift = pl.pallas_call(
        put_out,
        out_shape=shapes,
        in_specs=[pl.BlockSpec(memory_space=pl.ANY)] * 5,
        out_specs=(hbm,) * 5,
        scratch_shapes=[dma((5,))],
        compiler_params=pltpu.CompilerParams(vmem_limit_bytes=2**20),
        name="put_out",
    )(*results)
    return d_value, d_gate, d_taps, d_gain.reshape(WIDTH), d_shift.reshape(WIDTH)


def put_out(*refs):
    sems = refs[10]
    copies = [pltpu.make_async_copy(refs[i], refs[5 + i], sems.at[i]) for i in range(5)]
    for copy in copies:
        copy.start()
    for copy in copies:
        copy.wait()


def solution(mesh, dims=(12, 8, 4)):
    finer = Mesh(mesh.devices.reshape(*dims, mesh.shape["tp"]), (*SP, "tp"))
    total = ROWS * math.prod(dims)
    return jax.shard_map(
        functools.partial(shards, dims, total),
        mesh=finer,
        in_specs=(
            P(SP, "tp"), P(SP, "tp"), P(None, "tp"), P("tp"), P("tp"), P("tp", None), P(SP, None),
        ),
        out_specs=(P(SP, "tp"), P(SP, "tp"), P(None, "tp"), P("tp"), P("tp")),
        check_vma=False,
    )
```

```python
import functools
import math

import jax
import jax.numpy as jnp
from jax import lax
from jax.experimental import pallas as pl
from jax.experimental.pallas import tpu as pltpu
from jax.sharding import Mesh
from jax.sharding import PartitionSpec as P

SP = ("sp_0", "sp_1", "sp_2")
EPS = 1e-05
F32 = jnp.float32
BF16 = jnp.bfloat16
MESH = pl.DeviceIdType.MESH

ROWS, WIDTH, KERNEL, HALF = 256, 1024, 31, 15
ADDER = 1
REACH = (1, 2, 4)
ROUNDS = len(REACH) + 1
LANES, SUB, STEPS, PITCH, OUT_PITCH = 8, 8, 32, 72, 40
GROUP = 8


def position(dims):
    nz, ny, nx = dims
    z, y, x = (lax.axis_index(a) for a in SP)
    return z, y, x, lax.axis_index("tp"), (z * ny + y) * nx + x


def place(index, dims):
    nz, ny, nx = dims
    return {"sp_0": index // (ny * nx), "sp_1": (index // nx) % ny, "sp_2": index % nx}


def sigmoid(v):
    return jax.nn.sigmoid(v)


class Phases:
    def __init__(self):
        self.open = None

    def __call__(self, name):
        if self.open is not None:
            self.open.__exit__(None, None, None)
        self.open = None if name is None else jax.named_scope(name)
        if self.open is not None:
            self.open.__enter__()


def kernel(
    dims,
    total,
    value_hbm, gate_hbm, taps_hbm, gain_hbm, shift_hbm, w_hbm, cot_hbm,
    d_value, d_gate, d_taps, d_gain, d_shift,
    value, gate, taps, gain, shift, w, cot,
    gated, conv, mix, grad, wide, back, parts, bits,
    edge_out, edge_in, edge, tail_out, tail_in, tail,
    stat_out, stat_in, mean_b, inv_b, first_b, second_b,
    tiles, tiles_in, line, final, other, shift_x, shift_y, shift_z, spare,
    in_sem, w_sem, edge_send, edge_recv, stat_send, stat_recv, tail_send, tail_recv,
    rs_send, rs_recv, z_send, z_recv, ag_send, ag_recv, sh_send, sh_recv, rounds,
):
    nz, ny, nx = dims
    z, y, x, t, me = position(dims)
    n_sp = nz * ny * nx
    plane = ny * nx
    mine = x * ny + y
    after = place(lax.rem(me + 1, n_sp), dims)
    before = place(lax.rem(me + n_sp - 1, n_sp), dims)
    partner = {"tp": 1 - t}

    def far_first(count):
        return sorted(range(1, count), key=lambda step: -min(step, count - step))

    def ring(here, count):
        return [here] + [lax.rem(here + step, count) for step in range(1, count)]

    xs, ys, zs = ring(x, nx), ring(y, ny), ring(z, nz)
    in_plane = [
        {"sp_1": ys[dy], "sp_2": xs[dx]}
        for dx, dy in sorted(
            [(dx, dy) for dx in range(nx) for dy in range(ny) if dx or dy],
            key=lambda d: -(min(d[0], nx - d[0]) + min(d[1], ny - d[1])),
        )
    ]

    def along(axis, places):
        return [{axis: places[step]} for step in far_first(len(places))]

    phase = Phases()

    small = [
        pltpu.make_async_copy(src, dst, in_sem.at[i])
        for i, (src, dst) in enumerate(
            [(value_hbm, value), (gate_hbm, gate), (taps_hbm, taps), (gain_hbm, gain),
             (shift_hbm, shift), (cot_hbm, cot)]
        )
    ]
    big = [
        pltpu.make_async_copy(
            w_hbm.at[pl.ds(256 * i, 256)], w.at[pl.ds(256 * i, 256)], w_sem.at[i]
        )
        for i in range(4)
    ]
    for copy in small + big:
        copy.start()

    phase("greet")
    barrier = pltpu.get_barrier_semaphore()

    def greet(device):
        pl.semaphore_signal(barrier, inc=1, device_id=device, device_id_type=MESH)

    def core(device, which):
        return {**device, "tp": which}

    def at_distance(reach):
        found = []
        for axis, places in (("sp_2", xs), ("sp_1", ys), ("sp_0", zs)):
            count = len(places)
            if count > reach:
                found.append({axis: places[reach]})
                if count - reach > reach:
                    found.append({axis: places[-reach]})
        return found

    heard = [at_distance(reach) for reach in REACH] + [[partner]]
    for device in [after, before, partner] + heard[0]:
        greet(device)

    def tell(turn):
        for device in heard[turn]:
            pl.semaphore_signal(
                rounds.at[turn], inc=1, device_id=device, device_id_type=MESH
            )

    def hear(turn):
        pl.semaphore_wait(rounds.at[turn], len(heard[turn]))
        if turn + 1 < ROUNDS:
            tell(turn + 1)

    phase("load")
    small[0].wait()
    small[1].wait()

    def gated_of(rows, lanes):
        sig = sigmoid(gate[rows, lanes].astype(F32))
        return (value[rows, lanes].astype(F32) * sig).astype(BF16)

    phase("gate")
    for i, start in enumerate((0, ROWS - 16)):
        edge_out[i] = gated_of(pl.ds(start, 16), slice(None))

    starts = (PITCH, SUB * PITCH + 48)
    for l in range(LANES):
        for start in starts:
            gated[l, pl.ds(start, 16)] = jnp.zeros((16, 128), F32)
            wide[l, pl.ds(start, 16)] = jnp.zeros((16, 128), F32)
        edge[l, 16:32] = jnp.zeros((16, 128), F32)
        tail[l, 16:32] = jnp.zeros((16, 128), F32)

    @pl.loop(0, SUB)
    def _(s):
        for half in range(2):
            rows = pl.ds(pl.multiple_of(32 * s + 16 * half, 16), 16)
            for l in range(LANES):
                v = gated_of(rows, slice(128 * l, 128 * l + 128)).astype(F32)
                own = pl.multiple_of(PITCH * (s + 1) + 16 + 16 * half, 8)
                gated[l, pl.ds(own, 16)] = v
                other = pl.multiple_of(PITCH * s + 48 if half == 0 else PITCH * (s + 2), 8)
                gated[l, pl.ds(other, 16)] = v

    for i in (2, 3, 4):
        small[i].wait()

    def tap(k, l):
        lanes = pl.ds(pl.multiple_of(128 * l, 128), 128)
        return jnp.broadcast_to(taps[pl.ds(k, 1), lanes], (SUB, 128))

    def project(i):
        big[i].wait()
        product = lax.dot_general(
            cot[...], w[pl.ds(256 * i, 256)], (((1,), (1,)), ((), ())),
            preferred_element_type=F32,
        )
        for part in range(2):
            for s in range(SUB):
                mix[2 * i + part, pl.ds(OUT_PITCH * s, 32)] = product[
                    32 * s : 32 * s + 32, 128 * part : 128 * part + 128
                ]

    phase("conv")
    def convolve(l):
        for j0 in range(0, STEPS, GROUP):
            window = [
                gated[l, pl.ds(PITCH + j0 + 1 + i, SUB, stride=PITCH)]
                for i in range(GROUP + KERNEL - 1)
            ]
            sums = [jnp.zeros((SUB, 128), F32)] * GROUP
            for k in range(KERNEL):
                weight = tap(k, l)
                for i in range(GROUP):
                    sums[i] = sums[i] + weight * window[i + k]
            for i in range(GROUP):
                conv[l, pl.ds(8 * (j0 + i), 8)] = sums[i]

    pl.loop(0, LANES // 2)(convolve)

    phase("barrier")
    pl.semaphore_wait(barrier, 3 + len(heard[0]))
    tell(0)

    def exchange(source, target, send, recv, device):
        return pltpu.make_async_remote_copy(
            src_ref=source, dst_ref=target, send_sem=send, recv_sem=recv,
            device_id=device, device_id_type=MESH,
        )

    phase("edges")
    edges = [
        exchange(edge_out.at[0], edge_in.at[1], edge_send.at[0], edge_recv.at[1], before),
        exchange(edge_out.at[1], edge_in.at[0], edge_send.at[1], edge_recv.at[0], after),
    ]
    for copy in edges:
        copy.start()
    phase("conv2")
    pl.loop(LANES // 2, LANES)(convolve)
    hear(0)

    phase("project")
    small[5].wait()
    for i in range(3):
        project(i)
    hear(1)

    phase("edges_wait")
    for copy in edges:
        copy.wait()
    phase("fill")
    absent = (me == 0, me == n_sp - 1)
    for i in range(2):
        for l in range(LANES):
            v = edge_in[i, :, 128 * l : 128 * l + 128].astype(F32)
            v = jnp.where(absent[i], 0.0, v)
            gated[l, pl.ds(starts[i], 16)] = v
            edge[l, pl.ds(32 * i, 16)] = v

    @pl.loop(0, LANES)
    def _(l):
        for t0 in (0, 8):
            low = jnp.zeros((SUB, 128), F32)
            for k in range(HALF - t0):
                low = low + tap(k, l) * edge[l, pl.ds(t0 + k + 1, 8)]
            rows = pl.ds(8 * t0, 8, stride=8)
            conv[l, rows] = conv[l, rows] + low
            high = jnp.zeros((SUB, 128), F32)
            for k in range(24 - t0, KERNEL):
                high = high + tap(k, l) * edge[l, pl.ds(t0 + k + 1, 8)]
            rows = pl.ds(8 * (16 + t0) + 7, 8, stride=8)
            conv[l, rows] = conv[l, rows] + high

    lane = lax.broadcasted_iota(jnp.int32, (SUB, 128), 1)
    zero = jnp.zeros((SUB, 128), F32)

    def at_row(j):
        return pl.ds(pl.multiple_of(8 * j, 8), 8)

    def packed(ref):
        result = zero
        for j in range(STEPS):
            row = jnp.sum(ref[8 * j : 8 * j + 8], 1, keepdims=True)
            result = jnp.where(lane == j, row, result)
        return result

    def to_pair(slot):
        copy = exchange(
            stat_out.at[slot], stat_in.at[slot], stat_send.at[slot], stat_recv.at[slot], partner
        )
        copy.start()
        return copy

    def of_pair(copy, slot):
        copy.wait()
        return (
            stat_out[slot, 0] + stat_in[slot, 0],
            stat_out[slot, 1] + stat_in[slot, 1],
        )

    def spread(stat, target):
        for j in range(STEPS):
            target[8 * j : 8 * j + 8] = jnp.broadcast_to(stat[:, j : j + 1], (SUB, 128))

    phase("totals")

    @pl.loop(0, STEPS, unroll=4)
    def _(j):
        one, two = zero, zero
        for l in range(LANES):
            v = conv[l, at_row(j)]
            one = one + v
            two = two + v * v
        first_b[at_row(j)] = one
        second_b[at_row(j)] = two

    stat_out[0, 0] = packed(first_b)
    stat_out[0, 1] = packed(second_b)
    phase("pair0")
    copy = to_pair(0)
    project(3)
    phase("pair0_wait")
    one, two = of_pair(copy, 0)
    phase("spread0")
    width = 2.0 * WIDTH
    mean = one / width
    inv = lax.rsqrt(two / width - mean * mean + EPS)
    spread(mean, mean_b)
    spread(inv, inv_b)

    def norm(j, carry):
        by_gain, by_shift = (list(part) for part in carry)
        mean, inv = mean_b[at_row(j)], inv_b[at_row(j)]
        one, two = zero, zero
        for l in range(LANES):
            lanes = slice(128 * l, 128 * l + 128)
            g = gain[:, lanes]
            normed = (conv[l, at_row(j)] - mean) * inv
            pre = normed * g + shift[:, lanes]
            sig = sigmoid(pre)
            grad_pre = mix[l, pl.ds(j, SUB, stride=OUT_PITCH)] * sig * (1.0 + pre * (1.0 - sig))
            grad_normed = grad_pre * g
            one = one + grad_normed
            two = two + grad_normed * normed
            by_gain[l] = by_gain[l] + grad_pre * normed
            by_shift[l] = by_shift[l] + grad_pre
            conv[l, at_row(j)] = normed
            grad[l, at_row(j)] = grad_normed
        first_b[at_row(j)] = one
        second_b[at_row(j)] = two
        return tuple(by_gain), tuple(by_shift)

    phase("norm")
    by_gain, by_shift = lax.fori_loop(
        0, STEPS, norm, ((zero,) * LANES, (zero,) * LANES)
    )
    stat_out[1, 0] = packed(first_b)
    stat_out[1, 1] = packed(second_b)
    phase("pair1")
    copy = to_pair(1)
    hear(2)
    for l in range(LANES):
        parts[l, 8 * KERNEL : 8 * KERNEL + 8] = by_gain[l]
        spare[8 * l : 8 * l + 8] = by_shift[l]
    one, two = of_pair(copy, 1)
    phase("spread1")
    spread(one / width, first_b)
    spread(two / width, second_b)

    def folded(ref, start):
        rows = ref[pl.ds(start, 8, stride=8)]
        for s in range(1, SUB):
            rows = rows + ref[pl.ds(start + s, 8, stride=8)]
        return rows

    def to_axis(buffer, axis, places, index):
        own = buffer.at[places[0]]
        for device in along(axis, places):
            exchange(own, own, sh_send.at[index], sh_recv.at[index], device).start()

    def arrived(buffer, count, send, recv):
        if count > 1:
            some = buffer.at[pl.ds(0, count - 1)]
            pltpu.make_async_copy(some, some, recv).wait()
            pltpu.make_async_copy(some, some, send).wait()

    def from_axis(buffer, count, index):
        arrived(buffer, count, sh_send.at[index], sh_recv.at[index])
        result = buffer[0]
        for i in range(1, count):
            result = result + buffer[i]
        return result

    phase("shift_x")
    shift_x[x] = folded(spare, 0)
    to_axis(shift_x, "sp_2", xs, 0)

    def send_tile(g, l, device_x, device_y):
        q = g * LANES + l
        exchange(
            tiles.at[q], tiles_in.at[t * plane + mine], rs_send, rs_recv,
            {"sp_1": device_y, "sp_2": device_x, "tp": ADDER},
        ).start()

    def lane_block(i):
        odd = lax.rem(i, 2)
        offset = LANES // 2 + (i // 2) * (1 - odd) - ((i + 1) // 2) * odd
        return lax.rem(y + offset, LANES)

    hear(3)
    phase("taps")

    @pl.loop(0, LANES)
    def _(i):
        l = lane_block(i)
        for j in range(STEPS):
            rows = pl.ds(8 * j, 8)
            v = inv_b[rows] * (grad[l, rows] - first_b[rows] - conv[l, rows] * second_b[rows])
            grad[l, rows] = v
            wide[l, pl.ds(PITCH + 16 + j, SUB, stride=PITCH)] = v
            wide[l, pl.ds(j + 48 + 80 * (j // 16), SUB, stride=PITCH)] = v
        for k0 in range(0, KERNEL, GROUP):
            count = min(GROUP, KERNEL - k0)
            sums = [zero] * count
            window = [
                gated[l, pl.ds(PITCH + 1 + k0 + n, SUB, stride=PITCH)]
                for n in range(STEPS + count - 1)
            ]
            for j in range(STEPS):
                g = grad[l, pl.ds(8 * j, 8)]
                for n in range(count):
                    sums[n] = sums[n] + g * window[j + n]
            for n in range(count):
                parts[l, pl.ds(8 * (k0 + n), 8)] = sums[n]
        for g in range(4):
            tiles[g * LANES + l] = folded(parts.at[l], 64 * g)

        @pl.when(i > 0)
        def _():
            done = lane_block(i - 1)
            for step in (2, 1, 3, 0):
                send_tile(xs[step], done, xs[step], done)

    phase("rs_start")
    for step in far_first(nx):
        send_tile(xs[step], y, xs[step], y)

    @pl.when(t != ADDER)
    def _():
        send_tile(x, y, x, y)

    for l in range(LANES):
        tail_out[0, l] = wide[l, 48:64]
        tail_out[1, l] = wide[l, 9 * PITCH : 9 * PITCH + 16]
    shift_y[y] = from_axis(shift_x, nx, 0)
    to_axis(shift_y, "sp_1", ys, 1)
    tails = [
        exchange(tail_out.at[0], tail_in.at[1], tail_send.at[0], tail_recv.at[1], before),
        exchange(tail_out.at[1], tail_in.at[0], tail_send.at[1], tail_recv.at[0], after),
    ]
    for copy in tails:
        copy.start()

    phase("back")
    @pl.loop(0, LANES)
    def _(l):
        for j0 in range(0, STEPS, GROUP):
            low = PITCH + 31 - (KERNEL - 1) + j0
            window = [
                wide[l, pl.ds(low + i, SUB, stride=PITCH)] for i in range(GROUP + KERNEL - 1)
            ]
            sums = [zero] * GROUP
            for k in range(KERNEL):
                weight = tap(k, l)
                for i in range(GROUP):
                    sums[i] = sums[i] + weight * window[i + KERNEL - 1 - k]
            for i in range(GROUP):
                back[l, pl.ds(j0 + i, SUB, stride=OUT_PITCH)] = sums[i]

    def taken(sem, count):
        some = tiles_in.at[pl.ds(0, count)]
        pltpu.make_async_copy(some, some, sem).wait()

    phase("rs_wait")

    @pl.when(t == ADDER)
    def _():
        taken(rs_recv, 2 * plane - 1)
        tiles_in[ADDER * plane + mine] = tiles[mine]
        for which in range(2):
            halves = [tiles_in[which * plane], tiles_in[which * plane + 1]]
            for i in range(2, plane):
                halves[i % 2] = halves[i % 2] + tiles_in[which * plane + i]
            line[z, which] = halves[0] + halves[1]
        for device in along("sp_0", zs):
            exchange(line.at[z], line.at[z], z_send, z_recv, device).start()

    phase("shift_z")
    shift_z[z] = from_axis(shift_y, ny, 1)
    to_axis(shift_z, "sp_0", zs, 2)

    phase("tails")
    for copy in tails:
        copy.wait()
    for i in range(2):
        for l in range(LANES):
            tail[l, pl.ds(32 * i, 16)] = jnp.where(absent[i], 0.0, tail_in[i, l])

    @pl.loop(0, LANES)
    def _(l):
        for t0 in (0, 8):
            low = zero
            for k in range(16 + t0, KERNEL):
                low = low + tap(k, l) * tail[l, pl.ds(31 + t0 - k, 8)]
            rows = pl.ds(t0, 8)
            back[l, rows] = back[l, rows] + low
            high = zero
            for k in range(7 + t0):
                high = high + tap(k, l) * tail[l, pl.ds(31 + t0 - k, 8)]
            rows = pl.ds(OUT_PITCH * 7 + 16 + t0, 8)
            back[l, rows] = back[l, rows] + high

    phase("outputs")

    @pl.loop(0, SUB)
    def _(s):
        for half in range(2):
            rows = pl.ds(pl.multiple_of(32 * s + 16 * half, 16), 16)
            for l in range(LANES):
                lanes = slice(128 * l, 128 * l + 128)
                g = back[l, pl.ds(pl.multiple_of(OUT_PITCH * s + 16 * half, 8), 16)]
                sig = sigmoid(gate[rows, lanes].astype(F32))
                d_value[rows, lanes] = (g * sig).astype(BF16)
                d_gate[rows, lanes] = (
                    g * value[rows, lanes].astype(F32) * sig * (1.0 - sig)
                ).astype(BF16)

    phase("rs_wait")
    scale = 1.0 / math.sqrt(total)
    phase("z_wait")

    @pl.when(t == ADDER)
    def _():
        arrived(line, nz, z_send, z_recv)
        one, two = line[0, 0], line[0, 1]
        for i in range(1, nz):
            one, two = one + line[i, 0], two + line[i, 1]
        final[mine] = two * scale
        other[...] = one * scale
        for device in in_plane:
            exchange(other, final.at[mine], ag_send, ag_recv, core(device, 1 - ADDER)).start()
            exchange(
                final.at[mine], final.at[mine], ag_send, ag_recv, core(device, ADDER)
            ).start()
        exchange(other, final.at[mine], ag_send, ag_recv, partner).start()

    phase("shift_wait")
    d_shift[...] = from_axis(shift_z, nz, 2) * scale
    phase("ag_wait")

    @pl.when(t == ADDER)
    def _():
        taken(ag_recv, plane - 1)
        taken(ag_send, 2 * plane - 1)
        taken(rs_send, plane - 1)

    @pl.when(t != ADDER)
    def _():
        taken(ag_recv, plane)
        taken(rs_send, plane)

    phase("finish")
    for g in range(4):
        for l in range(LANES):
            lanes = slice(128 * l, 128 * l + 128)
            if g < 3:
                d_taps[8 * g : 8 * g + 8, lanes] = final[g * LANES + l]
            else:
                last = final[g * LANES + l]
                d_taps[24:KERNEL, lanes] = last[:7]
                d_gain[:, lanes] = last[7:]
    phase(None)


def shards(dims, total, value_in, gate_in, taps, gain, shift, w_out, grad_out):
    nz, ny, nx = dims
    depth = grad_out.shape[1]
    vmem = pltpu.VMEM
    dma = pltpu.SemaphoreType.DMA
    padded = (LANES, 10 * PITCH, 128)
    rows = (LANES, ROWS, 128)
    spread = (LANES, SUB * OUT_PITCH, 128)
    scratch = [
        vmem((ROWS, WIDTH), BF16), vmem((ROWS, WIDTH), BF16), vmem((KERNEL, WIDTH), F32),
        vmem((1, WIDTH), F32), vmem((1, WIDTH), F32), vmem((WIDTH, depth), BF16),
        vmem((ROWS, depth), BF16),
        vmem(padded, F32), vmem(rows, F32), vmem(spread, F32), vmem(rows, F32),
        vmem(padded, F32), vmem(spread, F32), vmem(rows, F32), vmem((8, 128), F32),
        vmem((2, 16, WIDTH), BF16), vmem((2, 16, WIDTH), BF16), vmem((LANES, 48, 128), F32),
        vmem((2, LANES, 16, 128), F32), vmem((2, LANES, 16, 128), F32),
        vmem((LANES, 48, 128), F32),
        vmem((2, 2, SUB, 128), F32), vmem((2, 2, SUB, 128), F32),
        vmem((ROWS, 128), F32), vmem((ROWS, 128), F32), vmem((ROWS, 128), F32),
        vmem((ROWS, 128), F32),
        vmem((32, 8, 128), F32), vmem((64, 8, 128), F32), vmem((nz, 2, 8, 128), F32),
        vmem((32, 8, 128), F32), vmem((8, 128), F32), vmem((nx, 8, 128), F32), vmem((ny, 8, 128), F32),
        vmem((nz, 8, 128), F32), vmem((64, 128), F32),
        dma((6,)), dma((4,)), dma((2,)), dma((2,)), dma((2,)), dma((2,)), dma((2,)), dma((2,)),
        dma, dma, dma, dma, dma, dma, dma((3,)), dma((3,)),
        pltpu.SemaphoreType.REGULAR((ROUNDS,)),
    ]
    hbm = pl.BlockSpec(memory_space=pltpu.HBM)
    near = pl.BlockSpec(memory_space=pltpu.VMEM)
    shape = jax.ShapeDtypeStruct
    shapes = (
        shape((ROWS, WIDTH), BF16), shape((ROWS, WIDTH), BF16), shape((KERNEL, WIDTH), F32),
        shape((1, WIDTH), F32), shape((8, 128), F32),
    )
    results = pl.pallas_call(
        functools.partial(kernel, dims, total),
        out_shape=shapes,
        in_specs=[hbm] * 7,
        out_specs=(near,) * 5,
        scratch_shapes=scratch,
        compiler_params=pltpu.CompilerParams(
            collective_id=0, has_side_effects=True, vmem_limit_bytes=40 * 2**20
        ),
        name="module",
    )(*(pltpu.with_memory_space_constraint(a, pltpu.HBM) for a in (value_in, gate_in, taps, gain.reshape(1, WIDTH), shift.reshape(1, WIDTH), w_out, grad_out)))
    d_value, d_gate, d_taps, d_gain, d_shift = pl.pallas_call(
        put_out,
        out_shape=shapes,
        in_specs=[pl.BlockSpec(memory_space=pl.ANY)] * 5,
        out_specs=(hbm,) * 5,
        scratch_shapes=[dma((5,))],
        compiler_params=pltpu.CompilerParams(vmem_limit_bytes=2**20),
        name="put_out",
    )(*results)
    return d_value, d_gate, d_taps, d_gain.reshape(WIDTH), d_shift.reshape(WIDTH)


def put_out(*refs):
    sems = refs[10]
    copies = [pltpu.make_async_copy(refs[i], refs[5 + i], sems.at[i]) for i in range(5)]
    for copy in copies:
        copy.start()
    for copy in copies:
        copy.wait()


def solution(mesh, dims=(12, 8, 4)):
    finer = Mesh(mesh.devices.reshape(*dims, mesh.shape["tp"]), (*SP, "tp"))
    total = ROWS * math.prod(dims)
    return jax.shard_map(
        functools.partial(shards, dims, total),
        mesh=finer,
        in_specs=(
            P(SP, "tp"), P(SP, "tp"), P(None, "tp"), P("tp"), P("tp"), P("tp", None), P(SP, None),
        ),
        out_specs=(P(SP, "tp"), P(SP, "tp"), P(None, "tp"), P("tp"), P("tp")),
        check_vma=False,
    )
```

```python
import functools
import math

import jax
import jax.numpy as jnp
from jax import lax
from jax.experimental import pallas as pl
from jax.experimental.pallas import tpu as pltpu
from jax.sharding import Mesh
from jax.sharding import PartitionSpec as P

SP = ("sp_0", "sp_1", "sp_2")
EPS = 1e-05
F32 = jnp.float32
BF16 = jnp.bfloat16
MESH = pl.DeviceIdType.MESH

ROWS, WIDTH, KERNEL, HALF = 256, 1024, 31, 15
ADDER = 1
REACH = (1, 2, 4)
ROUNDS = len(REACH) + 1
LANES, SUB, STEPS, PITCH, OUT_PITCH = 8, 8, 32, 72, 40
GROUP = 16
TAP_GROUP = 16


def position(dims):
    nz, ny, nx = dims
    z, y, x = (lax.axis_index(a) for a in SP)
    return z, y, x, lax.axis_index("tp"), (z * ny + y) * nx + x


def place(index, dims):
    nz, ny, nx = dims
    return {"sp_0": index // (ny * nx), "sp_1": (index // nx) % ny, "sp_2": index % nx}


def sigmoid(v):
    return jax.nn.sigmoid(v)


class Phases:
    def __init__(self):
        self.open = None

    def __call__(self, name):
        if self.open is not None:
            self.open.__exit__(None, None, None)
        self.open = None if name is None else jax.named_scope(name)
        if self.open is not None:
            self.open.__enter__()


def kernel(
    dims,
    total,
    value_hbm, gate_hbm, taps_hbm, gain_hbm, shift_hbm, w_hbm, cot_hbm,
    d_value, d_gate, d_taps, d_gain, d_shift,
    value, gate, taps, gain, shift, w, cot,
    gated, conv, mix, grad, wide, back, parts, bits,
    edge_out, edge_in, edge, tail_out, tail_in, tail,
    stat_out, stat_in, mean_b, inv_b, first_b, second_b, even, odd,
    tiles, tiles_in, line, final, other, shift_x, shift_y, shift_z, spare,
    in_sem, w_sem, edge_send, edge_recv, stat_send, stat_recv, tail_send, tail_recv,
    rs_send, rs_recv, z_send, z_recv, ag_send, ag_recv, sh_send, sh_recv, rounds,
):
    nz, ny, nx = dims
    z, y, x, t, me = position(dims)
    n_sp = nz * ny * nx
    plane = ny * nx
    mine = x * ny + y
    after = place(lax.rem(me + 1, n_sp), dims)
    before = place(lax.rem(me + n_sp - 1, n_sp), dims)
    partner = {"tp": 1 - t}

    def far_first(count):
        return sorted(range(1, count), key=lambda step: -min(step, count - step))

    def ring(here, count):
        return [here] + [lax.rem(here + step, count) for step in range(1, count)]

    xs, ys, zs = ring(x, nx), ring(y, ny), ring(z, nz)
    in_plane = [
        {"sp_1": ys[dy], "sp_2": xs[dx]}
        for dx, dy in sorted(
            [(dx, dy) for dx in range(nx) for dy in range(ny) if dx or dy],
            key=lambda d: -(min(d[0], nx - d[0]) + min(d[1], ny - d[1])),
        )
    ]

    def along(axis, places):
        return [{axis: places[step]} for step in far_first(len(places))]

    phase = Phases()

    small = [
        pltpu.make_async_copy(src, dst, in_sem.at[i])
        for i, (src, dst) in enumerate(
            [(value_hbm, value), (gate_hbm, gate), (taps_hbm, taps), (gain_hbm, gain),
             (shift_hbm, shift), (cot_hbm, cot)]
        )
    ]
    big = [
        pltpu.make_async_copy(
            w_hbm.at[pl.ds(256 * i, 256)], w.at[pl.ds(256 * i, 256)], w_sem.at[i]
        )
        for i in range(4)
    ]
    for copy in small + big:
        copy.start()

    phase("greet")
    barrier = pltpu.get_barrier_semaphore()

    def greet(device):
        pl.semaphore_signal(barrier, inc=1, device_id=device, device_id_type=MESH)

    def core(device, which):
        return {**device, "tp": which}

    def at_distance(reach):
        found = []
        for axis, places in (("sp_2", xs), ("sp_1", ys), ("sp_0", zs)):
            count = len(places)
            if count > reach:
                found.append({axis: places[reach]})
                if count - reach > reach:
                    found.append({axis: places[-reach]})
        return found

    heard = [at_distance(reach) for reach in REACH] + [[partner]]
    for device in [after, before, partner] + heard[0]:
        greet(device)

    def tell(turn):
        for device in heard[turn]:
            pl.semaphore_signal(
                rounds.at[turn], inc=1, device_id=device, device_id_type=MESH
            )

    def hear(turn):
        pl.semaphore_wait(rounds.at[turn], len(heard[turn]))
        if turn + 1 < ROUNDS:
            tell(turn + 1)

    phase("load")
    small[0].wait()
    small[1].wait()

    def gated_of(rows, lanes):
        sig = sigmoid(gate[rows, lanes].astype(F32))
        return (value[rows, lanes].astype(F32) * sig).astype(BF16)

    phase("gate")
    for i, start in enumerate((0, ROWS - 16)):
        edge_out[i] = gated_of(pl.ds(start, 16), slice(None))

    starts = (PITCH, SUB * PITCH + 48)
    for l in range(LANES):
        for start in starts:
            gated[l, pl.ds(start, 16)] = jnp.zeros((16, 128), F32)
            wide[l, pl.ds(start, 16)] = jnp.zeros((16, 128), F32)
        edge[l, 16:32] = jnp.zeros((16, 128), F32)
        tail[l, 16:32] = jnp.zeros((16, 128), F32)

    @pl.loop(0, SUB)
    def _(s):
        for half in range(2):
            rows = pl.ds(pl.multiple_of(32 * s + 16 * half, 16), 16)
            for l in range(LANES):
                v = gated_of(rows, slice(128 * l, 128 * l + 128)).astype(F32)
                own = pl.multiple_of(PITCH * (s + 1) + 16 + 16 * half, 8)
                gated[l, pl.ds(own, 16)] = v
                other = pl.multiple_of(PITCH * s + 48 if half == 0 else PITCH * (s + 2), 8)
                gated[l, pl.ds(other, 16)] = v

    for i in (2, 3, 4):
        small[i].wait()

    def tap(k, l):
        lanes = pl.ds(pl.multiple_of(128 * l, 128), 128)
        return jnp.broadcast_to(taps[pl.ds(k, 1), lanes], (SUB, 128))

    def project(i):
        big[i].wait()
        product = lax.dot_general(
            cot[...], w[pl.ds(256 * i, 256)], (((1,), (1,)), ((), ())),
            preferred_element_type=F32,
        )
        for part in range(2):
            for s in range(SUB):
                mix[2 * i + part, pl.ds(OUT_PITCH * s, 32)] = product[
                    32 * s : 32 * s + 32, 128 * part : 128 * part + 128
                ]

    phase("conv")
    def convolve(l):
        for j0 in range(0, STEPS, GROUP):
            window = [
                gated[l, pl.ds(PITCH + j0 + 1 + i, SUB, stride=PITCH)]
                for i in range(GROUP + KERNEL - 1)
            ]
            sums = [jnp.zeros((SUB, 128), F32)] * GROUP
            for k in range(KERNEL):
                weight = tap(k, l)
                for i in range(GROUP):
                    sums[i] = sums[i] + weight * window[i + k]
            for i in range(GROUP):
                conv[l, pl.ds(8 * (j0 + i), 8)] = sums[i]

    pl.loop(0, LANES // 2)(convolve)

    phase("barrier")
    pl.semaphore_wait(barrier, 3 + len(heard[0]))
    tell(0)

    def exchange(source, target, send, recv, device):
        return pltpu.make_async_remote_copy(
            src_ref=source, dst_ref=target, send_sem=send, recv_sem=recv,
            device_id=device, device_id_type=MESH,
        )

    phase("edges")
    edges = [
        exchange(edge_out.at[0], edge_in.at[1], edge_send.at[0], edge_recv.at[1], before),
        exchange(edge_out.at[1], edge_in.at[0], edge_send.at[1], edge_recv.at[0], after),
    ]
    for copy in edges:
        copy.start()
    phase("conv2")
    pl.loop(LANES // 2, LANES)(convolve)

    phase("project")
    small[5].wait()
    project(0)
    hear(0)
    project(1)
    project(2)

    phase("edges_wait")
    for copy in edges:
        copy.wait()
    phase("fill")
    absent = (me == 0, me == n_sp - 1)
    for i in range(2):
        for l in range(LANES):
            v = edge_in[i, :, 128 * l : 128 * l + 128].astype(F32)
            v = jnp.where(absent[i], 0.0, v)
            gated[l, pl.ds(starts[i], 16)] = v
            edge[l, pl.ds(32 * i, 16)] = v

    @pl.loop(0, LANES)
    def _(l):
        for t0 in (0, 8):
            low = jnp.zeros((SUB, 128), F32)
            for k in range(HALF - t0):
                low = low + tap(k, l) * edge[l, pl.ds(t0 + k + 1, 8)]
            rows = pl.ds(8 * t0, 8, stride=8)
            conv[l, rows] = conv[l, rows] + low
            high = jnp.zeros((SUB, 128), F32)
            for k in range(24 - t0, KERNEL):
                high = high + tap(k, l) * edge[l, pl.ds(t0 + k + 1, 8)]
            rows = pl.ds(8 * (16 + t0) + 7, 8, stride=8)
            conv[l, rows] = conv[l, rows] + high

    lane = lax.broadcasted_iota(jnp.int32, (SUB, 128), 1)
    zero = jnp.zeros((SUB, 128), F32)

    def at_row(j):
        return pl.ds(pl.multiple_of(8 * j, 8), 8)

    def packed(ref):
        result = zero
        for j in range(STEPS):
            row = jnp.sum(ref[8 * j : 8 * j + 8], 1, keepdims=True)
            result = jnp.where(lane == j, row, result)
        return result

    def to_pair(slot):
        copy = exchange(
            stat_out.at[slot], stat_in.at[slot], stat_send.at[slot], stat_recv.at[slot], partner
        )
        copy.start()
        return copy

    def of_pair(copy, slot):
        copy.wait()
        return (
            stat_out[slot, 0] + stat_in[slot, 0],
            stat_out[slot, 1] + stat_in[slot, 1],
        )

    def spread(stat, target):
        for j in range(STEPS):
            target[8 * j : 8 * j + 8] = jnp.broadcast_to(stat[:, j : j + 1], (SUB, 128))

    phase("totals")

    @pl.loop(0, STEPS, unroll=4)
    def _(j):
        one, two = zero, zero
        for l in range(LANES):
            v = conv[l, at_row(j)]
            one = one + v
            two = two + v * v
        first_b[at_row(j)] = one
        second_b[at_row(j)] = two

    stat_out[0, 0] = packed(first_b)
    stat_out[0, 1] = packed(second_b)
    phase("pair0")
    copy = to_pair(0)
    hear(1)
    project(3)
    phase("pair0_wait")
    one, two = of_pair(copy, 0)
    phase("spread0")
    width = 2.0 * WIDTH
    mean = one / width
    inv = lax.rsqrt(two / width - mean * mean + EPS)
    spread(mean, mean_b)
    spread(inv, inv_b)

    def norm(j, carry):
        by_gain, by_shift = (list(part) for part in carry)
        mean, inv = mean_b[at_row(j)], inv_b[at_row(j)]
        one, two = zero, zero
        for l in range(LANES):
            lanes = slice(128 * l, 128 * l + 128)
            g = gain[:, lanes]
            normed = (conv[l, at_row(j)] - mean) * inv
            pre = normed * g + shift[:, lanes]
            sig = sigmoid(pre)
            grad_pre = mix[l, pl.ds(j, SUB, stride=OUT_PITCH)] * sig * (1.0 + pre * (1.0 - sig))
            grad_normed = grad_pre * g
            one = one + grad_normed
            two = two + grad_normed * normed
            by_gain[l] = by_gain[l] + grad_pre * normed
            by_shift[l] = by_shift[l] + grad_pre
            conv[l, at_row(j)] = normed
            grad[l, at_row(j)] = grad_normed
        first_b[at_row(j)] = one
        second_b[at_row(j)] = two
        return tuple(by_gain), tuple(by_shift)

    phase("norm")
    by_gain, by_shift = lax.fori_loop(
        0, STEPS, norm, ((zero,) * LANES, (zero,) * LANES), unroll=2
    )
    stat_out[1, 0] = packed(first_b)
    stat_out[1, 1] = packed(second_b)
    phase("pair1")
    copy = to_pair(1)
    hear(2)
    for l in range(LANES):
        parts[l, 8 * KERNEL : 8 * KERNEL + 8] = by_gain[l]
        spare[8 * l : 8 * l + 8] = by_shift[l]
    one, two = of_pair(copy, 1)
    phase("spread1")
    spread(one / width, first_b)
    spread(two / width, second_b)

    def folded(ref, start):
        rows = ref[pl.ds(start, 8, stride=8)]
        for s in range(1, SUB):
            rows = rows + ref[pl.ds(start + s, 8, stride=8)]
        return rows

    def to_axis(buffer, axis, places, index):
        own = buffer.at[places[0]]
        for device in along(axis, places):
            exchange(own, own, sh_send.at[index], sh_recv.at[index], device).start()

    def arrived(buffer, count, send, recv):
        if count > 1:
            some = buffer.at[pl.ds(0, count - 1)]
            pltpu.make_async_copy(some, some, recv).wait()
            pltpu.make_async_copy(some, some, send).wait()

    def from_axis(buffer, count, index):
        arrived(buffer, count, sh_send.at[index], sh_recv.at[index])
        result = buffer[0]
        for i in range(1, count):
            result = result + buffer[i]
        return result

    phase("shift_x")
    shift_x[x] = folded(spare, 0)
    to_axis(shift_x, "sp_2", xs, 0)

    def send_tile(g, l, device_x, device_y):
        q = g * LANES + l
        exchange(
            tiles.at[q], tiles_in.at[t * plane + mine], rs_send, rs_recv,
            {"sp_1": device_y, "sp_2": device_x, "tp": ADDER},
        ).start()

    def lane_block(i):
        odd = lax.rem(i, 2)
        offset = LANES // 2 + (i // 2) * (1 - odd) - ((i + 1) // 2) * odd
        return lax.rem(y + offset, LANES)

    hear(3)
    phase("taps")

    def grad_conv(l, target, steps):
        for j in steps:
            rows = pl.ds(8 * j, 8)
            v = inv_b[rows] * (grad[l, rows] - first_b[rows] - conv[l, rows] * second_b[rows])
            target[rows] = v
            wide[l, pl.ds(PITCH + 16 + j, SUB, stride=PITCH)] = v
            wide[l, pl.ds(j + 48 + 80 * (j // 16), SUB, stride=PITCH)] = v

    def tap_sums(l, source, meanwhile):
        for k0 in range(0, KERNEL, TAP_GROUP):
            count = min(TAP_GROUP, KERNEL - k0)
            sums = [zero] * count
            window = [
                gated[l, pl.ds(PITCH + 1 + k0 + n, SUB, stride=PITCH)]
                for n in range(STEPS + count - 1)
            ]
            for j in range(STEPS):
                g = source[8 * j : 8 * j + 8]
                for n in range(count):
                    sums[n] = sums[n] + g * window[j + n]
                if j % 2:
                    meanwhile(k0 + j // 2)
            for n in range(count):
                parts[l, pl.ds(8 * (k0 + n), 8)] = sums[n]
        for g in range(4):
            tiles[g * LANES + l] = folded(parts.at[l], 64 * g)

    def send_tiles(l):
        for step in (2, 1, 3, 0):
            send_tile(xs[step], l, xs[step], l)

    grad_conv(lane_block(0), even, range(STEPS))

    @pl.loop(0, LANES // 2)
    def _(pair):
        for n, (now, then) in enumerate(((even, odd), (odd, even))):
            i = 2 * pair + n
            coming = lane_block(i + 1)
            tap_sums(lane_block(i), now, lambda j: grad_conv(coming, then, [j]))
            if n:
                send_tiles(lane_block(i - 1))
            else:

                @pl.when(pair > 0)
                def _():
                    send_tiles(lane_block(i - 1))

    phase("rs_start")
    for step in far_first(nx):
        send_tile(xs[step], y, xs[step], y)

    @pl.when(t != ADDER)
    def _():
        send_tile(x, y, x, y)

    for l in range(LANES):
        tail_out[0, l] = wide[l, 48:64]
        tail_out[1, l] = wide[l, 9 * PITCH : 9 * PITCH + 16]
    shift_y[y] = from_axis(shift_x, nx, 0)
    to_axis(shift_y, "sp_1", ys, 1)
    tails = [
        exchange(tail_out.at[0], tail_in.at[1], tail_send.at[0], tail_recv.at[1], before),
        exchange(tail_out.at[1], tail_in.at[0], tail_send.at[1], tail_recv.at[0], after),
    ]
    for copy in tails:
        copy.start()

    phase("back")
    @pl.loop(0, LANES)
    def _(l):
        for j0 in range(0, STEPS, GROUP):
            low = PITCH + 31 - (KERNEL - 1) + j0
            window = [
                wide[l, pl.ds(low + i, SUB, stride=PITCH)] for i in range(GROUP + KERNEL - 1)
            ]
            sums = [zero] * GROUP
            for k in range(KERNEL):
                weight = tap(k, l)
                for i in range(GROUP):
                    sums[i] = sums[i] + weight * window[i + KERNEL - 1 - k]
            for i in range(GROUP):
                back[l, pl.ds(j0 + i, SUB, stride=OUT_PITCH)] = sums[i]

    def taken(sem, count):
        some = tiles_in.at[pl.ds(0, count)]
        pltpu.make_async_copy(some, some, sem).wait()

    phase("rs_wait")

    @pl.when(t == ADDER)
    def _():
        taken(rs_recv, 2 * plane - 1)
        tiles_in[ADDER * plane + mine] = tiles[mine]
        for which in range(2):
            halves = [tiles_in[which * plane], tiles_in[which * plane + 1]]
            for i in range(2, plane):
                halves[i % 2] = halves[i % 2] + tiles_in[which * plane + i]
            line[z, which] = halves[0] + halves[1]
        for device in along("sp_0", zs):
            exchange(line.at[z], line.at[z], z_send, z_recv, device).start()

    phase("shift_z")
    shift_z[z] = from_axis(shift_y, ny, 1)
    to_axis(shift_z, "sp_0", zs, 2)

    phase("tails")
    for copy in tails:
        copy.wait()
    for i in range(2):
        for l in range(LANES):
            tail[l, pl.ds(32 * i, 16)] = jnp.where(absent[i], 0.0, tail_in[i, l])

    @pl.loop(0, LANES)
    def _(l):
        for t0 in (0, 8):
            low = zero
            for k in range(16 + t0, KERNEL):
                low = low + tap(k, l) * tail[l, pl.ds(31 + t0 - k, 8)]
            rows = pl.ds(t0, 8)
            back[l, rows] = back[l, rows] + low
            high = zero
            for k in range(7 + t0):
                high = high + tap(k, l) * tail[l, pl.ds(31 + t0 - k, 8)]
            rows = pl.ds(OUT_PITCH * 7 + 16 + t0, 8)
            back[l, rows] = back[l, rows] + high

    phase("outputs")

    @pl.loop(0, SUB)
    def _(s):
        for half in range(2):
            rows = pl.ds(pl.multiple_of(32 * s + 16 * half, 16), 16)
            for l in range(LANES):
                lanes = slice(128 * l, 128 * l + 128)
                g = back[l, pl.ds(pl.multiple_of(OUT_PITCH * s + 16 * half, 8), 16)]
                sig = sigmoid(gate[rows, lanes].astype(F32))
                d_value[rows, lanes] = (g * sig).astype(BF16)
                d_gate[rows, lanes] = (
                    g * value[rows, lanes].astype(F32) * sig * (1.0 - sig)
                ).astype(BF16)

    phase("rs_wait")
    scale = 1.0 / math.sqrt(total)
    phase("z_wait")

    @pl.when(t == ADDER)
    def _():
        arrived(line, nz, z_send, z_recv)
        one, two = line[0, 0], line[0, 1]
        for i in range(1, nz):
            one, two = one + line[i, 0], two + line[i, 1]
        final[mine] = two * scale
        other[...] = one * scale
        for device in in_plane:
            exchange(other, final.at[mine], ag_send, ag_recv, core(device, 1 - ADDER)).start()
            exchange(
                final.at[mine], final.at[mine], ag_send, ag_recv, core(device, ADDER)
            ).start()
        exchange(other, final.at[mine], ag_send, ag_recv, partner).start()

    phase("shift_wait")
    d_shift[...] = from_axis(shift_z, nz, 2) * scale
    phase("ag_wait")

    @pl.when(t == ADDER)
    def _():
        taken(ag_recv, plane - 1)
        taken(ag_send, 2 * plane - 1)
        taken(rs_send, plane - 1)

    @pl.when(t != ADDER)
    def _():
        taken(ag_recv, plane)
        taken(rs_send, plane)

    phase("finish")
    for g in range(4):
        for l in range(LANES):
            lanes = slice(128 * l, 128 * l + 128)
            if g < 3:
                d_taps[8 * g : 8 * g + 8, lanes] = final[g * LANES + l]
            else:
                last = final[g * LANES + l]
                d_taps[24:KERNEL, lanes] = last[:7]
                d_gain[:, lanes] = last[7:]
    phase(None)


def shards(dims, total, value_in, gate_in, taps, gain, shift, w_out, grad_out):
    nz, ny, nx = dims
    depth = grad_out.shape[1]
    vmem = pltpu.VMEM
    dma = pltpu.SemaphoreType.DMA
    padded = (LANES, 10 * PITCH, 128)
    rows = (LANES, ROWS, 128)
    spread = (LANES, SUB * OUT_PITCH, 128)
    scratch = [
        vmem((ROWS, WIDTH), BF16), vmem((ROWS, WIDTH), BF16), vmem((KERNEL, WIDTH), F32),
        vmem((1, WIDTH), F32), vmem((1, WIDTH), F32), vmem((WIDTH, depth), BF16),
        vmem((ROWS, depth), BF16),
        vmem(padded, F32), vmem(rows, F32), vmem(spread, F32), vmem(rows, F32),
        vmem(padded, F32), vmem(spread, F32), vmem(rows, F32), vmem((8, 128), F32),
        vmem((2, 16, WIDTH), BF16), vmem((2, 16, WIDTH), BF16), vmem((LANES, 48, 128), F32),
        vmem((2, LANES, 16, 128), F32), vmem((2, LANES, 16, 128), F32),
        vmem((LANES, 48, 128), F32),
        vmem((2, 2, SUB, 128), F32), vmem((2, 2, SUB, 128), F32),
        vmem((ROWS, 128), F32), vmem((ROWS, 128), F32), vmem((ROWS, 128), F32),
        vmem((ROWS, 128), F32), vmem((ROWS, 128), F32), vmem((ROWS, 128), F32),
        vmem((32, 8, 128), F32), vmem((64, 8, 128), F32), vmem((nz, 2, 8, 128), F32),
        vmem((32, 8, 128), F32), vmem((8, 128), F32), vmem((nx, 8, 128), F32), vmem((ny, 8, 128), F32),
        vmem((nz, 8, 128), F32), vmem((64, 128), F32),
        dma((6,)), dma((4,)), dma((2,)), dma((2,)), dma((2,)), dma((2,)), dma((2,)), dma((2,)),
        dma, dma, dma, dma, dma, dma, dma((3,)), dma((3,)),
        pltpu.SemaphoreType.REGULAR((ROUNDS,)),
    ]
    hbm = pl.BlockSpec(memory_space=pltpu.HBM)
    near = pl.BlockSpec(memory_space=pltpu.VMEM)
    shape = jax.ShapeDtypeStruct
    shapes = (
        shape((ROWS, WIDTH), BF16), shape((ROWS, WIDTH), BF16), shape((KERNEL, WIDTH), F32),
        shape((1, WIDTH), F32), shape((8, 128), F32),
    )
    results = pl.pallas_call(
        functools.partial(kernel, dims, total),
        out_shape=shapes,
        in_specs=[hbm] * 7,
        out_specs=(near,) * 5,
        scratch_shapes=scratch,
        compiler_params=pltpu.CompilerParams(
            collective_id=0, has_side_effects=True, vmem_limit_bytes=40 * 2**20
        ),
        name="module",
    )(*(pltpu.with_memory_space_constraint(a, pltpu.HBM) for a in (value_in, gate_in, taps, gain.reshape(1, WIDTH), shift.reshape(1, WIDTH), w_out, grad_out)))
    d_value, d_gate, d_taps, d_gain, d_shift = pl.pallas_call(
        put_out,
        out_shape=shapes,
        in_specs=[pl.BlockSpec(memory_space=pl.ANY)] * 5,
        out_specs=(hbm,) * 5,
        scratch_shapes=[dma((11,))],
        compiler_params=pltpu.CompilerParams(vmem_limit_bytes=2**20),
        name="put_out",
    )(*results)
    return d_value, d_gate, d_taps, d_gain.reshape(WIDTH), d_shift.reshape(WIDTH)


def put_out(*refs):
    sems = refs[10]
    pieces = [(i, pl.ds(64 * n, 64)) for n in range(4) for i in range(2)]
    pieces += [(i, slice(None)) for i in range(2, 5)]
    copies = [
        pltpu.make_async_copy(refs[i].at[rows], refs[5 + i].at[rows], sems.at[n])
        for n, (i, rows) in enumerate(pieces)
    ]
    for copy in copies:
        copy.start()
    for copy in copies:
        copy.wait()


def solution(mesh, dims=(12, 8, 4)):
    finer = Mesh(mesh.devices.reshape(*dims, mesh.shape["tp"]), (*SP, "tp"))
    total = ROWS * math.prod(dims)
    return jax.shard_map(
        functools.partial(shards, dims, total),
        mesh=finer,
        in_specs=(
            P(SP, "tp"), P(SP, "tp"), P(None, "tp"), P("tp"), P("tp"), P("tp", None), P(SP, None),
        ),
        out_specs=(P(SP, "tp"), P(SP, "tp"), P(None, "tp"), P("tp"), P("tp")),
        check_vma=False,
    )
```

```python
import functools
import math

import jax
import jax.numpy as jnp
from jax import lax
from jax.experimental import pallas as pl
from jax.experimental.pallas import tpu as pltpu
from jax.sharding import Mesh
from jax.sharding import PartitionSpec as P

SP = ("sp_0", "sp_1", "sp_2")
EPS = 1e-05
F32 = jnp.float32
BF16 = jnp.bfloat16
MESH = pl.DeviceIdType.MESH

ROWS, WIDTH, KERNEL, HALF = 256, 1024, 31, 15
ADDER = 1
REACH = (1, 2, 4)
ROUNDS = len(REACH) + 1
LANES, SUB, STEPS, PITCH, OUT_PITCH = 8, 8, 32, 72, 40
GROUP = 16
TAP_GROUP = 16


def position(dims):
    nz, ny, nx = dims
    z, y, x = (lax.axis_index(a) for a in SP)
    return z, y, x, lax.axis_index("tp"), (z * ny + y) * nx + x


def place(index, dims):
    nz, ny, nx = dims
    return {"sp_0": index // (ny * nx), "sp_1": (index // nx) % ny, "sp_2": index % nx}


def sigmoid(v):
    return jax.nn.sigmoid(v)


class Phases:
    def __init__(self):
        self.open = None

    def __call__(self, name):
        if self.open is not None:
            self.open.__exit__(None, None, None)
        self.open = None if name is None else jax.named_scope(name)
        if self.open is not None:
            self.open.__enter__()


def kernel(
    dims,
    total,
    value_hbm, gate_hbm, taps_hbm, gain_hbm, shift_hbm, w_hbm, cot_hbm,
    d_value, d_gate, d_taps, d_gain, d_shift,
    value, gate, taps, gain, shift, w, cot,
    gated, conv, mix, grad, wide, back, parts, bits,
    edge_out, edge_in, edge, tail_out, tail_in, tail,
    stat_out, stat_in, mean_b, inv_b, first_b, second_b, even, odd,
    tiles, tiles_in, line, final, other, shift_x, shift_y, shift_z, spare,
    in_sem, w_sem, edge_send, edge_recv, stat_send, stat_recv, tail_send, tail_recv,
    rs_send, rs_recv, z_send, z_recv, ag_send, ag_recv, sh_send, sh_recv, rounds,
):
    nz, ny, nx = dims
    z, y, x, t, me = position(dims)
    n_sp = nz * ny * nx
    plane = ny * nx
    mine = x * ny + y
    after = place(lax.rem(me + 1, n_sp), dims)
    before = place(lax.rem(me + n_sp - 1, n_sp), dims)
    partner = {"tp": 1 - t}

    def far_first(count):
        return sorted(range(1, count), key=lambda step: -min(step, count - step))

    def ring(here, count):
        return [here] + [lax.rem(here + step, count) for step in range(1, count)]

    xs, ys, zs = ring(x, nx), ring(y, ny), ring(z, nz)
    in_plane = [
        {"sp_1": ys[dy], "sp_2": xs[dx]}
        for dx, dy in sorted(
            [(dx, dy) for dx in range(nx) for dy in range(ny) if dx or dy],
            key=lambda d: -(min(d[0], nx - d[0]) + min(d[1], ny - d[1])),
        )
    ]

    def along(axis, places):
        return [{axis: places[step]} for step in far_first(len(places))]

    phase = Phases()

    small = [
        pltpu.make_async_copy(src, dst, in_sem.at[i])
        for i, (src, dst) in enumerate(
            [(value_hbm, value), (gate_hbm, gate), (taps_hbm, taps), (gain_hbm, gain),
             (shift_hbm, shift), (cot_hbm, cot)]
        )
    ]
    big = [
        pltpu.make_async_copy(
            w_hbm.at[pl.ds(256 * i, 256)], w.at[pl.ds(256 * i, 256)], w_sem.at[i]
        )
        for i in range(4)
    ]
    for copy in small + big:
        copy.start()

    phase("greet")
    barrier = pltpu.get_barrier_semaphore()

    def greet(device):
        pl.semaphore_signal(barrier, inc=1, device_id=device, device_id_type=MESH)

    def core(device, which):
        return {**device, "tp": which}

    def at_distance(reach):
        found = []
        for axis, places in (("sp_2", xs), ("sp_1", ys), ("sp_0", zs)):
            count = len(places)
            if count > reach:
                found.append({axis: places[reach]})
                if count - reach > reach:
                    found.append({axis: places[-reach]})
        return found

    heard = [at_distance(reach) for reach in REACH] + [[partner]]
    for device in [after, before, partner] + heard[0]:
        greet(device)

    def tell(turn):
        for device in heard[turn]:
            pl.semaphore_signal(
                rounds.at[turn], inc=1, device_id=device, device_id_type=MESH
            )

    def hear(turn):
        pl.semaphore_wait(rounds.at[turn], len(heard[turn]))
        if turn + 1 < ROUNDS:
            tell(turn + 1)

    phase("load")
    small[0].wait()
    small[1].wait()

    def gated_of(rows, lanes):
        sig = sigmoid(gate[rows, lanes].astype(F32))
        return (value[rows, lanes].astype(F32) * sig).astype(BF16)

    phase("gate")
    for i, start in enumerate((0, ROWS - 16)):
        edge_out[i] = gated_of(pl.ds(start, 16), slice(None))

    starts = (PITCH, SUB * PITCH + 48)
    for l in range(LANES):
        for start in starts:
            gated[l, pl.ds(start, 16)] = jnp.zeros((16, 128), F32)
            wide[l, pl.ds(start, 16)] = jnp.zeros((16, 128), F32)
        edge[l, 16:32] = jnp.zeros((16, 128), F32)
        tail[l, 16:32] = jnp.zeros((16, 128), F32)

    @pl.loop(0, SUB)
    def _(s):
        for half in range(2):
            rows = pl.ds(pl.multiple_of(32 * s + 16 * half, 16), 16)
            for l in range(LANES):
                v = gated_of(rows, slice(128 * l, 128 * l + 128)).astype(F32)
                own = pl.multiple_of(PITCH * (s + 1) + 16 + 16 * half, 8)
                gated[l, pl.ds(own, 16)] = v
                other = pl.multiple_of(PITCH * s + 48 if half == 0 else PITCH * (s + 2), 8)
                gated[l, pl.ds(other, 16)] = v

    for i in (2, 3, 4):
        small[i].wait()

    def tap(k, l):
        lanes = pl.ds(pl.multiple_of(128 * l, 128), 128)
        return jnp.broadcast_to(taps[pl.ds(k, 1), lanes], (SUB, 128))

    def project(i):
        big[i].wait()
        product = lax.dot_general(
            cot[...], w[pl.ds(256 * i, 256)], (((1,), (1,)), ((), ())),
            preferred_element_type=F32,
        )
        for part in range(2):
            for s in range(SUB):
                mix[2 * i + part, pl.ds(OUT_PITCH * s, 32)] = product[
                    32 * s : 32 * s + 32, 128 * part : 128 * part + 128
                ]

    phase("conv")
    def convolve(l):
        for j0 in range(0, STEPS, GROUP):
            window = [
                gated[l, pl.ds(PITCH + j0 + 1 + i, SUB, stride=PITCH)]
                for i in range(GROUP + KERNEL - 1)
            ]
            sums = [jnp.zeros((SUB, 128), F32)] * GROUP
            for k in range(KERNEL):
                weight = tap(k, l)
                for i in range(GROUP):
                    sums[i] = sums[i] + weight * window[i + k]
            for i in range(GROUP):
                conv[l, pl.ds(8 * (j0 + i), 8)] = sums[i]

    pl.loop(0, LANES // 2)(convolve)

    phase("barrier")
    pl.semaphore_wait(barrier, 3 + len(heard[0]))
    tell(0)

    def exchange(source, target, send, recv, device):
        return pltpu.make_async_remote_copy(
            src_ref=source, dst_ref=target, send_sem=send, recv_sem=recv,
            device_id=device, device_id_type=MESH,
        )

    phase("edges")
    edges = [
        exchange(edge_out.at[0], edge_in.at[1], edge_send.at[0], edge_recv.at[1], before),
        exchange(edge_out.at[1], edge_in.at[0], edge_send.at[1], edge_recv.at[0], after),
    ]
    for copy in edges:
        copy.start()
    phase("conv2")
    pl.loop(LANES // 2, LANES)(convolve)

    phase("project")
    small[5].wait()
    project(0)
    hear(0)
    project(1)
    project(2)
    hear(1)

    phase("edges_wait")
    for copy in edges:
        copy.wait()
    phase("fill")
    absent = (me == 0, me == n_sp - 1)
    for i in range(2):
        for l in range(LANES):
            v = edge_in[i, :, 128 * l : 128 * l + 128].astype(F32)
            v = jnp.where(absent[i], 0.0, v)
            gated[l, pl.ds(starts[i], 16)] = v
            edge[l, pl.ds(32 * i, 16)] = v

    @pl.loop(0, LANES)
    def _(l):
        for t0 in (0, 8):
            low = jnp.zeros((SUB, 128), F32)
            for k in range(HALF - t0):
                low = low + tap(k, l) * edge[l, pl.ds(t0 + k + 1, 8)]
            rows = pl.ds(8 * t0, 8, stride=8)
            conv[l, rows] = conv[l, rows] + low
            high = jnp.zeros((SUB, 128), F32)
            for k in range(24 - t0, KERNEL):
                high = high + tap(k, l) * edge[l, pl.ds(t0 + k + 1, 8)]
            rows = pl.ds(8 * (16 + t0) + 7, 8, stride=8)
            conv[l, rows] = conv[l, rows] + high

    lane = lax.broadcasted_iota(jnp.int32, (SUB, 128), 1)
    zero = jnp.zeros((SUB, 128), F32)

    def at_row(j):
        return pl.ds(pl.multiple_of(8 * j, 8), 8)

    def packed(ref):
        result = zero
        for j in range(STEPS):
            row = jnp.sum(ref[8 * j : 8 * j + 8], 1, keepdims=True)
            result = jnp.where(lane == j, row, result)
        return result

    def to_pair(slot):
        copy = exchange(
            stat_out.at[slot], stat_in.at[slot], stat_send.at[slot], stat_recv.at[slot], partner
        )
        copy.start()
        return copy

    def of_pair(copy, slot):
        copy.wait()
        return (
            stat_out[slot, 0] + stat_in[slot, 0],
            stat_out[slot, 1] + stat_in[slot, 1],
        )

    def spread(stat, target):
        for j in range(STEPS):
            target[8 * j : 8 * j + 8] = jnp.broadcast_to(stat[:, j : j + 1], (SUB, 128))

    phase("totals")

    @pl.loop(0, STEPS, unroll=4)
    def _(j):
        one, two = zero, zero
        for l in range(LANES):
            v = conv[l, at_row(j)]
            one = one + v
            two = two + v * v
        first_b[at_row(j)] = one
        second_b[at_row(j)] = two

    stat_out[0, 0] = packed(first_b)
    stat_out[0, 1] = packed(second_b)
    phase("pair0")
    copy = to_pair(0)
    project(3)
    phase("pair0_wait")
    one, two = of_pair(copy, 0)
    phase("spread0")
    width = 2.0 * WIDTH
    mean = one / width
    inv = lax.rsqrt(two / width - mean * mean + EPS)
    spread(mean, mean_b)
    spread(inv, inv_b)

    def norm(j, carry):
        by_gain, by_shift = (list(part) for part in carry)
        mean, inv = mean_b[at_row(j)], inv_b[at_row(j)]
        one, two = zero, zero
        for l in range(LANES):
            lanes = slice(128 * l, 128 * l + 128)
            g = gain[:, lanes]
            normed = (conv[l, at_row(j)] - mean) * inv
            pre = normed * g + shift[:, lanes]
            sig = sigmoid(pre)
            grad_pre = mix[l, pl.ds(j, SUB, stride=OUT_PITCH)] * sig * (1.0 + pre * (1.0 - sig))
            grad_normed = grad_pre * g
            one = one + grad_normed
            two = two + grad_normed * normed
            by_gain[l] = by_gain[l] + grad_pre * normed
            by_shift[l] = by_shift[l] + grad_pre
            conv[l, at_row(j)] = normed
            grad[l, at_row(j)] = grad_normed
        first_b[at_row(j)] = one
        second_b[at_row(j)] = two
        return tuple(by_gain), tuple(by_shift)

    phase("norm")
    by_gain, by_shift = lax.fori_loop(
        0, STEPS, norm, ((zero,) * LANES, (zero,) * LANES), unroll=2
    )
    stat_out[1, 0] = packed(first_b)
    stat_out[1, 1] = packed(second_b)
    phase("pair1")
    copy = to_pair(1)
    for l in range(LANES):
        parts[l, 8 * KERNEL : 8 * KERNEL + 8] = by_gain[l]
        spare[8 * l : 8 * l + 8] = by_shift[l]
    one, two = of_pair(copy, 1)
    phase("spread1")
    spread(one / width, first_b)
    spread(two / width, second_b)

    def folded(ref, start):
        rows = ref[pl.ds(start, 8, stride=8)]
        for s in range(1, SUB):
            rows = rows + ref[pl.ds(start + s, 8, stride=8)]
        return rows

    def to_axis(buffer, axis, places, index):
        own = buffer.at[places[0]]
        for device in along(axis, places):
            exchange(own, own, sh_send.at[index], sh_recv.at[index], device).start()

    def arrived(buffer, count, send, recv):
        if count > 1:
            some = buffer.at[pl.ds(0, count - 1)]
            pltpu.make_async_copy(some, some, recv).wait()
            pltpu.make_async_copy(some, some, send).wait()

    def from_axis(buffer, count, index):
        arrived(buffer, count, sh_send.at[index], sh_recv.at[index])
        result = buffer[0]
        for i in range(1, count):
            result = result + buffer[i]
        return result

    phase("shift_x")
    shift_x[x] = folded(spare, 0)
    to_axis(shift_x, "sp_2", xs, 0)

    def send_tile(g, l, device_x, device_y):
        q = g * LANES + l
        exchange(
            tiles.at[q], tiles_in.at[t * plane + mine], rs_send, rs_recv,
            {"sp_1": device_y, "sp_2": device_x, "tp": ADDER},
        ).start()

    def lane_block(i):
        odd = lax.rem(i, 2)
        offset = LANES // 2 + (i // 2) * (1 - odd) - ((i + 1) // 2) * odd
        return lax.rem(y + offset, LANES)

    hear(2)
    phase("taps")

    def grad_conv(l, target, steps):
        for j in steps:
            rows = pl.ds(8 * j, 8)
            v = inv_b[rows] * (grad[l, rows] - first_b[rows] - conv[l, rows] * second_b[rows])
            target[rows] = v
            wide[l, pl.ds(PITCH + 16 + j, SUB, stride=PITCH)] = v
            wide[l, pl.ds(j + 48 + 80 * (j // 16), SUB, stride=PITCH)] = v

    def tap_sums(l, source, meanwhile):
        for k0 in range(0, KERNEL, TAP_GROUP):
            count = min(TAP_GROUP, KERNEL - k0)
            sums = [zero] * count
            window = [
                gated[l, pl.ds(PITCH + 1 + k0 + n, SUB, stride=PITCH)]
                for n in range(STEPS + count - 1)
            ]
            for j in range(STEPS):
                g = source[8 * j : 8 * j + 8]
                for n in range(count):
                    sums[n] = sums[n] + g * window[j + n]
                if j % 2:
                    meanwhile(k0 + j // 2)
            for n in range(count):
                parts[l, pl.ds(8 * (k0 + n), 8)] = sums[n]
        for g in range(4):
            tiles[g * LANES + l] = folded(parts.at[l], 64 * g)

    def send_tiles(l):
        for step in (2, 1, 3, 0):
            send_tile(xs[step], l, xs[step], l)

    grad_conv(lane_block(0), even, range(STEPS))

    @pl.loop(0, LANES // 2)
    def _(pair):
        for n, (now, then) in enumerate(((even, odd), (odd, even))):
            i = 2 * pair + n
            coming = lane_block(i + 1)
            tap_sums(lane_block(i), now, lambda j: grad_conv(coming, then, [j]))
            if n:

                @pl.when(pair == 0)
                def _():
                    hear(3)

                send_tiles(lane_block(i - 1))
            else:

                @pl.when(pair > 0)
                def _():
                    send_tiles(lane_block(i - 1))

    phase("rs_start")
    for step in far_first(nx):
        send_tile(xs[step], y, xs[step], y)

    @pl.when(t != ADDER)
    def _():
        send_tile(x, y, x, y)

    for l in range(LANES):
        tail_out[0, l] = wide[l, 48:64]
        tail_out[1, l] = wide[l, 9 * PITCH : 9 * PITCH + 16]
    shift_y[y] = from_axis(shift_x, nx, 0)
    to_axis(shift_y, "sp_1", ys, 1)
    tails = [
        exchange(tail_out.at[0], tail_in.at[1], tail_send.at[0], tail_recv.at[1], before),
        exchange(tail_out.at[1], tail_in.at[0], tail_send.at[1], tail_recv.at[0], after),
    ]
    for copy in tails:
        copy.start()

    phase("back")
    @pl.loop(0, LANES)
    def _(l):
        for j0 in range(0, STEPS, GROUP):
            low = PITCH + 31 - (KERNEL - 1) + j0
            window = [
                wide[l, pl.ds(low + i, SUB, stride=PITCH)] for i in range(GROUP + KERNEL - 1)
            ]
            sums = [zero] * GROUP
            for k in range(KERNEL):
                weight = tap(k, l)
                for i in range(GROUP):
                    sums[i] = sums[i] + weight * window[i + KERNEL - 1 - k]
            for i in range(GROUP):
                back[l, pl.ds(j0 + i, SUB, stride=OUT_PITCH)] = sums[i]

    def taken(sem, count):
        some = tiles_in.at[pl.ds(0, count)]
        pltpu.make_async_copy(some, some, sem).wait()

    phase("rs_wait")

    @pl.when(t == ADDER)
    def _():
        taken(rs_recv, 2 * plane - 1)
        tiles_in[ADDER * plane + mine] = tiles[mine]
        for which in range(2):
            halves = [tiles_in[which * plane], tiles_in[which * plane + 1]]
            for i in range(2, plane):
                halves[i % 2] = halves[i % 2] + tiles_in[which * plane + i]
            line[z, which] = halves[0] + halves[1]
        for device in along("sp_0", zs):
            exchange(line.at[z], line.at[z], z_send, z_recv, device).start()

    phase("shift_z")
    shift_z[z] = from_axis(shift_y, ny, 1)
    to_axis(shift_z, "sp_0", zs, 2)

    phase("tails")
    for copy in tails:
        copy.wait()
    for i in range(2):
        for l in range(LANES):
            tail[l, pl.ds(32 * i, 16)] = jnp.where(absent[i], 0.0, tail_in[i, l])

    @pl.loop(0, LANES)
    def _(l):
        for t0 in (0, 8):
            low = zero
            for k in range(16 + t0, KERNEL):
                low = low + tap(k, l) * tail[l, pl.ds(31 + t0 - k, 8)]
            rows = pl.ds(t0, 8)
            back[l, rows] = back[l, rows] + low
            high = zero
            for k in range(7 + t0):
                high = high + tap(k, l) * tail[l, pl.ds(31 + t0 - k, 8)]
            rows = pl.ds(OUT_PITCH * 7 + 16 + t0, 8)
            back[l, rows] = back[l, rows] + high

    phase("outputs")

    @pl.loop(0, SUB)
    def _(s):
        for half in range(2):
            rows = pl.ds(pl.multiple_of(32 * s + 16 * half, 16), 16)
            for l in range(LANES):
                lanes = slice(128 * l, 128 * l + 128)
                g = back[l, pl.ds(pl.multiple_of(OUT_PITCH * s + 16 * half, 8), 16)]
                sig = sigmoid(gate[rows, lanes].astype(F32))
                d_value[rows, lanes] = (g * sig).astype(BF16)
                d_gate[rows, lanes] = (
                    g * value[rows, lanes].astype(F32) * sig * (1.0 - sig)
                ).astype(BF16)

    phase("rs_wait")
    scale = 1.0 / math.sqrt(total)
    phase("z_wait")

    @pl.when(t == ADDER)
    def _():
        arrived(line, nz, z_send, z_recv)
        one, two = line[0, 0], line[0, 1]
        for i in range(1, nz):
            one, two = one + line[i, 0], two + line[i, 1]
        final[mine] = two * scale
        other[...] = one * scale
        for device in in_plane:
            exchange(other, final.at[mine], ag_send, ag_recv, core(device, 1 - ADDER)).start()
            exchange(
                final.at[mine], final.at[mine], ag_send, ag_recv, core(device, ADDER)
            ).start()
        exchange(other, final.at[mine], ag_send, ag_recv, partner).start()

    phase("shift_wait")
    d_shift[...] = from_axis(shift_z, nz, 2) * scale
    phase("ag_wait")

    @pl.when(t == ADDER)
    def _():
        taken(ag_recv, plane - 1)
        taken(ag_send, 2 * plane - 1)
        taken(rs_send, plane - 1)

    @pl.when(t != ADDER)
    def _():
        taken(ag_recv, plane)
        taken(rs_send, plane)

    phase("finish")
    for g in range(4):
        for l in range(LANES):
            lanes = slice(128 * l, 128 * l + 128)
            if g < 3:
                d_taps[8 * g : 8 * g + 8, lanes] = final[g * LANES + l]
            else:
                last = final[g * LANES + l]
                d_taps[24:KERNEL, lanes] = last[:7]
                d_gain[:, lanes] = last[7:]
    phase(None)


def shards(dims, total, value_in, gate_in, taps, gain, shift, w_out, grad_out):
    nz, ny, nx = dims
    depth = grad_out.shape[1]
    vmem = pltpu.VMEM
    dma = pltpu.SemaphoreType.DMA
    padded = (LANES, 10 * PITCH, 128)
    rows = (LANES, ROWS, 128)
    spread = (LANES, SUB * OUT_PITCH, 128)
    scratch = [
        vmem((ROWS, WIDTH), BF16), vmem((ROWS, WIDTH), BF16), vmem((KERNEL, WIDTH), F32),
        vmem((1, WIDTH), F32), vmem((1, WIDTH), F32), vmem((WIDTH, depth), BF16),
        vmem((ROWS, depth), BF16),
        vmem(padded, F32), vmem(rows, F32), vmem(spread, F32), vmem(rows, F32),
        vmem(padded, F32), vmem(spread, F32), vmem(rows, F32), vmem((8, 128), F32),
        vmem((2, 16, WIDTH), BF16), vmem((2, 16, WIDTH), BF16), vmem((LANES, 48, 128), F32),
        vmem((2, LANES, 16, 128), F32), vmem((2, LANES, 16, 128), F32),
        vmem((LANES, 48, 128), F32),
        vmem((2, 2, SUB, 128), F32), vmem((2, 2, SUB, 128), F32),
        vmem((ROWS, 128), F32), vmem((ROWS, 128), F32), vmem((ROWS, 128), F32),
        vmem((ROWS, 128), F32), vmem((ROWS, 128), F32), vmem((ROWS, 128), F32),
        vmem((32, 8, 128), F32), vmem((64, 8, 128), F32), vmem((nz, 2, 8, 128), F32),
        vmem((32, 8, 128), F32), vmem((8, 128), F32), vmem((nx, 8, 128), F32), vmem((ny, 8, 128), F32),
        vmem((nz, 8, 128), F32), vmem((64, 128), F32),
        dma((6,)), dma((4,)), dma((2,)), dma((2,)), dma((2,)), dma((2,)), dma((2,)), dma((2,)),
        dma, dma, dma, dma, dma, dma, dma((3,)), dma((3,)),
        pltpu.SemaphoreType.REGULAR((ROUNDS,)),
    ]
    hbm = pl.BlockSpec(memory_space=pltpu.HBM)
    near = pl.BlockSpec(memory_space=pltpu.VMEM)
    shape = jax.ShapeDtypeStruct
    shapes = (
        shape((ROWS, WIDTH), BF16), shape((ROWS, WIDTH), BF16), shape((KERNEL, WIDTH), F32),
        shape((1, WIDTH), F32), shape((8, 128), F32),
    )
    results = pl.pallas_call(
        functools.partial(kernel, dims, total),
        out_shape=shapes,
        in_specs=[hbm] * 7,
        out_specs=(near,) * 5,
        scratch_shapes=scratch,
        compiler_params=pltpu.CompilerParams(
            collective_id=0, has_side_effects=True, vmem_limit_bytes=40 * 2**20
        ),
        name="module",
    )(*(pltpu.with_memory_space_constraint(a, pltpu.HBM) for a in (value_in, gate_in, taps, gain.reshape(1, WIDTH), shift.reshape(1, WIDTH), w_out, grad_out)))
    d_value, d_gate, d_taps, d_gain, d_shift = pl.pallas_call(
        put_out,
        out_shape=shapes,
        in_specs=[pl.BlockSpec(memory_space=pl.ANY)] * 5,
        out_specs=(hbm,) * 5,
        scratch_shapes=[dma((5,))],
        compiler_params=pltpu.CompilerParams(vmem_limit_bytes=2**20),
        name="put_out",
    )(*results)
    return d_value, d_gate, d_taps, d_gain.reshape(WIDTH), d_shift.reshape(WIDTH)


def put_out(*refs):
    sems = refs[10]
    copies = [pltpu.make_async_copy(refs[i], refs[5 + i], sems.at[i]) for i in range(5)]
    for copy in copies:
        copy.start()
    for copy in copies:
        copy.wait()


def solution(mesh, dims=(12, 8, 4)):
    finer = Mesh(mesh.devices.reshape(*dims, mesh.shape["tp"]), (*SP, "tp"))
    total = ROWS * math.prod(dims)
    return jax.shard_map(
        functools.partial(shards, dims, total),
        mesh=finer,
        in_specs=(
            P(SP, "tp"), P(SP, "tp"), P(None, "tp"), P("tp"), P("tp"), P("tp", None), P(SP, None),
        ),
        out_specs=(P(SP, "tp"), P(SP, "tp"), P(None, "tp"), P("tp"), P("tp")),
        check_vma=False,
    )
```

```python
import functools
import math

import jax
import jax.numpy as jnp
from jax import lax
from jax.experimental import pallas as pl
from jax.experimental.pallas import tpu as pltpu
from jax.sharding import Mesh
from jax.sharding import PartitionSpec as P

SP = ("sp_0", "sp_1", "sp_2")
EPS = 1e-05
F32 = jnp.float32
BF16 = jnp.bfloat16
MESH = pl.DeviceIdType.MESH

ROWS, WIDTH, KERNEL, HALF = 256, 1024, 31, 15
ADDER = 1
REACH = (1, 2, 4)
ROUNDS = len(REACH) + 1
LANES, SUB, STEPS, PITCH, OUT_PITCH = 8, 8, 32, 72, 40
GROUP = 16
TAP_GROUP = 16


def position(dims):
    nz, ny, nx = dims
    z, y, x = (lax.axis_index(a) for a in SP)
    return z, y, x, lax.axis_index("tp"), (z * ny + y) * nx + x


def place(index, dims):
    nz, ny, nx = dims
    return {"sp_0": index // (ny * nx), "sp_1": (index // nx) % ny, "sp_2": index % nx}


def sigmoid(v):
    return jax.nn.sigmoid(v)


class Phases:
    def __init__(self):
        self.open = None

    def __call__(self, name):
        if self.open is not None:
            self.open.__exit__(None, None, None)
        self.open = None if name is None else jax.named_scope(name)
        if self.open is not None:
            self.open.__enter__()


def kernel(
    dims,
    total,
    value_hbm, gate_hbm, taps_hbm, gain_hbm, shift_hbm, w_hbm, cot_hbm,
    d_value, d_gate, d_taps, d_gain, d_shift,
    value, gate, taps, gain, shift, w, cot,
    gated, conv, mix, grad, wide, back, parts, bits,
    edge_out, edge_in, edge, tail_out, tail_in, tail,
    stat_out, stat_in, mean_b, inv_b, first_b, second_b, even, odd,
    tiles, tiles_in, line, final, other, shift_x, shift_y, shift_z, spare,
    in_sem, w_sem, edge_send, edge_recv, stat_send, stat_recv, tail_send, tail_recv,
    rs_send, rs_recv, z_send, z_recv, ag_send, ag_recv, sh_send, sh_recv, rounds,
):
    nz, ny, nx = dims
    z, y, x, t, me = position(dims)
    n_sp = nz * ny * nx
    plane = ny * nx
    mine = x * ny + y
    after = place(lax.rem(me + 1, n_sp), dims)
    before = place(lax.rem(me + n_sp - 1, n_sp), dims)
    partner = {"tp": 1 - t}

    def far_first(count):
        return sorted(range(1, count), key=lambda step: -min(step, count - step))

    def ring(here, count):
        return [here] + [lax.rem(here + step, count) for step in range(1, count)]

    xs, ys, zs = ring(x, nx), ring(y, ny), ring(z, nz)
    in_plane = [
        {"sp_1": ys[dy], "sp_2": xs[dx]}
        for dx, dy in sorted(
            [(dx, dy) for dx in range(nx) for dy in range(ny) if dx or dy],
            key=lambda d: -(min(d[0], nx - d[0]) + min(d[1], ny - d[1])),
        )
    ]

    def along(axis, places):
        return [{axis: places[step]} for step in far_first(len(places))]

    phase = Phases()

    small = [
        pltpu.make_async_copy(src, dst, in_sem.at[i])
        for i, (src, dst) in enumerate(
            [(value_hbm, value), (gate_hbm, gate), (taps_hbm, taps), (gain_hbm, gain),
             (shift_hbm, shift), (cot_hbm, cot)]
        )
    ]
    big = [
        pltpu.make_async_copy(
            w_hbm.at[pl.ds(256 * i, 256)], w.at[pl.ds(256 * i, 256)], w_sem.at[i]
        )
        for i in range(4)
    ]
    for copy in small + big:
        copy.start()

    phase("greet")
    barrier = pltpu.get_barrier_semaphore()

    def greet(device):
        pl.semaphore_signal(barrier, inc=1, device_id=device, device_id_type=MESH)

    def core(device, which):
        return {**device, "tp": which}

    def at_distance(reach):
        found = []
        for axis, places in (("sp_2", xs), ("sp_1", ys), ("sp_0", zs)):
            count = len(places)
            if count > reach:
                found.append({axis: places[reach]})
                if count - reach > reach:
                    found.append({axis: places[-reach]})
        return found

    heard = [at_distance(reach) for reach in REACH] + [[partner]]
    for device in [after, before, partner] + heard[0]:
        greet(device)

    def tell(turn):
        for device in heard[turn]:
            pl.semaphore_signal(
                rounds.at[turn], inc=1, device_id=device, device_id_type=MESH
            )

    def hear(turn):
        pl.semaphore_wait(rounds.at[turn], len(heard[turn]))
        if turn + 1 < ROUNDS:
            tell(turn + 1)

    phase("load")
    small[0].wait()
    small[1].wait()

    def gated_of(rows, lanes):
        sig = sigmoid(gate[rows, lanes].astype(F32))
        return (value[rows, lanes].astype(F32) * sig).astype(BF16)

    phase("gate")
    for i, start in enumerate((0, ROWS - 16)):
        edge_out[i] = gated_of(pl.ds(start, 16), slice(None))

    starts = (PITCH, SUB * PITCH + 48)
    for l in range(LANES):
        for start in starts:
            gated[l, pl.ds(start, 16)] = jnp.zeros((16, 128), F32)
            wide[l, pl.ds(start, 16)] = jnp.zeros((16, 128), F32)
        edge[l, 16:32] = jnp.zeros((16, 128), F32)
        tail[l, 16:32] = jnp.zeros((16, 128), F32)

    @pl.loop(0, SUB)
    def _(s):
        for half in range(2):
            rows = pl.ds(pl.multiple_of(32 * s + 16 * half, 16), 16)
            for l in range(LANES):
                v = gated_of(rows, slice(128 * l, 128 * l + 128)).astype(F32)
                own = pl.multiple_of(PITCH * (s + 1) + 16 + 16 * half, 8)
                gated[l, pl.ds(own, 16)] = v
                other = pl.multiple_of(PITCH * s + 48 if half == 0 else PITCH * (s + 2), 8)
                gated[l, pl.ds(other, 16)] = v

    for i in (2, 3, 4):
        small[i].wait()

    def tap(k, l):
        lanes = pl.ds(pl.multiple_of(128 * l, 128), 128)
        return jnp.broadcast_to(taps[pl.ds(k, 1), lanes], (SUB, 128))

    def project(i):
        big[i].wait()
        product = lax.dot_general(
            cot[...], w[pl.ds(256 * i, 256)], (((1,), (1,)), ((), ())),
            preferred_element_type=F32,
        )
        for part in range(2):
            for s in range(SUB):
                mix[2 * i + part, pl.ds(OUT_PITCH * s, 32)] = product[
                    32 * s : 32 * s + 32, 128 * part : 128 * part + 128
                ]

    phase("conv")
    def convolve(l):
        for j0 in range(0, STEPS, GROUP):
            window = [
                gated[l, pl.ds(PITCH + j0 + 1 + i, SUB, stride=PITCH)]
                for i in range(GROUP + KERNEL - 1)
            ]
            sums = [jnp.zeros((SUB, 128), F32)] * GROUP
            for k in range(KERNEL):
                weight = tap(k, l)
                for i in range(GROUP):
                    sums[i] = sums[i] + weight * window[i + k]
            for i in range(GROUP):
                conv[l, pl.ds(8 * (j0 + i), 8)] = sums[i]

    pl.loop(0, LANES // 2)(convolve)

    phase("barrier")
    pl.semaphore_wait(barrier, 3 + len(heard[0]))
    tell(0)

    def exchange(source, target, send, recv, device):
        return pltpu.make_async_remote_copy(
            src_ref=source, dst_ref=target, send_sem=send, recv_sem=recv,
            device_id=device, device_id_type=MESH,
        )

    phase("edges")
    edges = [
        exchange(edge_out.at[0], edge_in.at[1], edge_send.at[0], edge_recv.at[1], before),
        exchange(edge_out.at[1], edge_in.at[0], edge_send.at[1], edge_recv.at[0], after),
    ]
    for copy in edges:
        copy.start()
    phase("conv2")
    pl.loop(LANES // 2, LANES)(convolve)

    phase("project")
    small[5].wait()
    project(0)
    hear(0)
    project(1)
    project(2)
    hear(1)

    phase("edges_wait")
    for copy in edges:
        copy.wait()
    phase("fill")
    absent = (me == 0, me == n_sp - 1)
    for i in range(2):
        for l in range(LANES):
            v = edge_in[i, :, 128 * l : 128 * l + 128].astype(F32)
            v = jnp.where(absent[i], 0.0, v)
            gated[l, pl.ds(starts[i], 16)] = v
            edge[l, pl.ds(32 * i, 16)] = v

    @pl.loop(0, LANES, unroll=2)
    def _(l):
        for t0 in (0, 8):
            low = jnp.zeros((SUB, 128), F32)
            for k in range(HALF - t0):
                low = low + tap(k, l) * edge[l, pl.ds(t0 + k + 1, 8)]
            rows = pl.ds(8 * t0, 8, stride=8)
            conv[l, rows] = conv[l, rows] + low
            high = jnp.zeros((SUB, 128), F32)
            for k in range(24 - t0, KERNEL):
                high = high + tap(k, l) * edge[l, pl.ds(t0 + k + 1, 8)]
            rows = pl.ds(8 * (16 + t0) + 7, 8, stride=8)
            conv[l, rows] = conv[l, rows] + high

    lane = lax.broadcasted_iota(jnp.int32, (SUB, 128), 1)
    zero = jnp.zeros((SUB, 128), F32)

    def at_row(j):
        return pl.ds(pl.multiple_of(8 * j, 8), 8)

    def packed(ref):
        result = zero
        for j in range(STEPS):
            row = jnp.sum(ref[8 * j : 8 * j + 8], 1, keepdims=True)
            result = jnp.where(lane == j, row, result)
        return result

    def to_pair(slot):
        copy = exchange(
            stat_out.at[slot], stat_in.at[slot], stat_send.at[slot], stat_recv.at[slot], partner
        )
        copy.start()
        return copy

    def of_pair(copy, slot):
        copy.wait()
        return (
            stat_out[slot, 0] + stat_in[slot, 0],
            stat_out[slot, 1] + stat_in[slot, 1],
        )

    def spread(stat, target):
        for j in range(STEPS):
            target[8 * j : 8 * j + 8] = jnp.broadcast_to(stat[:, j : j + 1], (SUB, 128))

    phase("totals")

    @pl.loop(0, STEPS, unroll=4)
    def _(j):
        one, two = zero, zero
        for l in range(LANES):
            v = conv[l, at_row(j)]
            one = one + v
            two = two + v * v
        first_b[at_row(j)] = one
        second_b[at_row(j)] = two

    stat_out[0, 0] = packed(first_b)
    stat_out[0, 1] = packed(second_b)
    phase("pair0")
    copy = to_pair(0)
    project(3)
    phase("pair0_wait")
    one, two = of_pair(copy, 0)
    phase("spread0")
    width = 2.0 * WIDTH
    mean = one / width
    inv = lax.rsqrt(two / width - mean * mean + EPS)
    spread(mean, mean_b)
    spread(inv, inv_b)

    def norm(j, carry):
        by_gain, by_shift = (list(part) for part in carry)
        mean, inv = mean_b[at_row(j)], inv_b[at_row(j)]
        one, two = zero, zero
        for l in range(LANES):
            lanes = slice(128 * l, 128 * l + 128)
            g = gain[:, lanes]
            normed = (conv[l, at_row(j)] - mean) * inv
            pre = normed * g + shift[:, lanes]
            sig = sigmoid(pre)
            grad_pre = mix[l, pl.ds(j, SUB, stride=OUT_PITCH)] * sig * (1.0 + pre * (1.0 - sig))
            grad_normed = grad_pre * g
            one = one + grad_normed
            two = two + grad_normed * normed
            by_gain[l] = by_gain[l] + grad_pre * normed
            by_shift[l] = by_shift[l] + grad_pre
            conv[l, at_row(j)] = normed
            grad[l, at_row(j)] = grad_normed
        first_b[at_row(j)] = one
        second_b[at_row(j)] = two
        return tuple(by_gain), tuple(by_shift)

    phase("norm")
    by_gain, by_shift = lax.fori_loop(
        0, STEPS, norm, ((zero,) * LANES, (zero,) * LANES), unroll=4
    )
    stat_out[1, 0] = packed(first_b)
    stat_out[1, 1] = packed(second_b)
    phase("pair1")
    copy = to_pair(1)
    for l in range(LANES):
        parts[l, 8 * KERNEL : 8 * KERNEL + 8] = by_gain[l]
        spare[8 * l : 8 * l + 8] = by_shift[l]
    one, two = of_pair(copy, 1)
    phase("spread1")
    spread(one / width, first_b)
    spread(two / width, second_b)

    def folded(ref, start):
        rows = ref[pl.ds(start, 8, stride=8)]
        for s in range(1, SUB):
            rows = rows + ref[pl.ds(start + s, 8, stride=8)]
        return rows

    def to_axis(buffer, axis, places, index):
        own = buffer.at[places[0]]
        for device in along(axis, places):
            exchange(own, own, sh_send.at[index], sh_recv.at[index], device).start()

    def arrived(buffer, count, send, recv):
        if count > 1:
            some = buffer.at[pl.ds(0, count - 1)]
            pltpu.make_async_copy(some, some, recv).wait()
            pltpu.make_async_copy(some, some, send).wait()

    def from_axis(buffer, count, index):
        arrived(buffer, count, sh_send.at[index], sh_recv.at[index])
        result = buffer[0]
        for i in range(1, count):
            result = result + buffer[i]
        return result

    phase("shift_x")
    shift_x[x] = folded(spare, 0)
    to_axis(shift_x, "sp_2", xs, 0)

    def send_tile(g, l, device_x, device_y):
        q = g * LANES + l
        exchange(
            tiles.at[q], tiles_in.at[t * plane + mine], rs_send, rs_recv,
            {"sp_1": device_y, "sp_2": device_x, "tp": ADDER},
        ).start()

    def lane_block(i):
        odd = lax.rem(i, 2)
        offset = LANES // 2 + (i // 2) * (1 - odd) - ((i + 1) // 2) * odd
        return lax.rem(y + offset, LANES)

    hear(2)
    phase("taps")

    def grad_conv(l, target, steps):
        for j in steps:
            rows = pl.ds(8 * j, 8)
            v = inv_b[rows] * (grad[l, rows] - first_b[rows] - conv[l, rows] * second_b[rows])
            target[rows] = v
            wide[l, pl.ds(PITCH + 16 + j, SUB, stride=PITCH)] = v
            wide[l, pl.ds(j + 48 + 80 * (j // 16), SUB, stride=PITCH)] = v

    def tap_sums(l, source, meanwhile):
        for k0 in range(0, KERNEL, TAP_GROUP):
            count = min(TAP_GROUP, KERNEL - k0)
            sums = [zero] * count
            window = [
                gated[l, pl.ds(PITCH + 1 + k0 + n, SUB, stride=PITCH)]
                for n in range(STEPS + count - 1)
            ]
            for j in range(STEPS):
                g = source[8 * j : 8 * j + 8]
                for n in range(count):
                    sums[n] = sums[n] + g * window[j + n]
                if j % 2:
                    meanwhile(k0 + j // 2)
            for n in range(count):
                parts[l, pl.ds(8 * (k0 + n), 8)] = sums[n]
        for g in range(4):
            tiles[g * LANES + l] = folded(parts.at[l], 64 * g)

    def send_tiles(l):
        for step in (2, 1, 3, 0):
            send_tile(xs[step], l, xs[step], l)

    grad_conv(lane_block(0), even, range(STEPS))

    @pl.loop(0, LANES // 2)
    def _(pair):
        for n, (now, then) in enumerate(((even, odd), (odd, even))):
            i = 2 * pair + n
            coming = lane_block(i + 1)
            tap_sums(lane_block(i), now, lambda j: grad_conv(coming, then, [j]))
            if n:

                @pl.when(pair == 0)
                def _():
                    hear(3)

                send_tiles(lane_block(i - 1))
            else:

                @pl.when(pair > 0)
                def _():
                    send_tiles(lane_block(i - 1))

    phase("rs_start")
    for step in far_first(nx):
        send_tile(xs[step], y, xs[step], y)

    @pl.when(t != ADDER)
    def _():
        send_tile(x, y, x, y)

    for l in range(LANES):
        tail_out[0, l] = wide[l, 48:64]
        tail_out[1, l] = wide[l, 9 * PITCH : 9 * PITCH + 16]
    shift_y[y] = from_axis(shift_x, nx, 0)
    to_axis(shift_y, "sp_1", ys, 1)
    tails = [
        exchange(tail_out.at[0], tail_in.at[1], tail_send.at[0], tail_recv.at[1], before),
        exchange(tail_out.at[1], tail_in.at[0], tail_send.at[1], tail_recv.at[0], after),
    ]
    for copy in tails:
        copy.start()

    phase("back")
    @pl.loop(0, LANES)
    def _(l):
        for j0 in range(0, STEPS, GROUP):
            low = PITCH + 31 - (KERNEL - 1) + j0
            window = [
                wide[l, pl.ds(low + i, SUB, stride=PITCH)] for i in range(GROUP + KERNEL - 1)
            ]
            sums = [zero] * GROUP
            for k in range(KERNEL):
                weight = tap(k, l)
                for i in range(GROUP):
                    sums[i] = sums[i] + weight * window[i + KERNEL - 1 - k]
            for i in range(GROUP):
                back[l, pl.ds(j0 + i, SUB, stride=OUT_PITCH)] = sums[i]

    def taken(sem, count):
        some = tiles_in.at[pl.ds(0, count)]
        pltpu.make_async_copy(some, some, sem).wait()

    phase("rs_wait")

    @pl.when(t == ADDER)
    def _():
        taken(rs_recv, 2 * plane - 1)
        tiles_in[ADDER * plane + mine] = tiles[mine]
        for which in range(2):
            halves = [tiles_in[which * plane], tiles_in[which * plane + 1]]
            for i in range(2, plane):
                halves[i % 2] = halves[i % 2] + tiles_in[which * plane + i]
            line[z, which] = halves[0] + halves[1]
        for device in along("sp_0", zs):
            exchange(line.at[z], line.at[z], z_send, z_recv, device).start()

    phase("shift_z")
    shift_z[z] = from_axis(shift_y, ny, 1)
    to_axis(shift_z, "sp_0", zs, 2)

    phase("tails")
    for copy in tails:
        copy.wait()
    for i in range(2):
        for l in range(LANES):
            tail[l, pl.ds(32 * i, 16)] = jnp.where(absent[i], 0.0, tail_in[i, l])

    @pl.loop(0, LANES)
    def _(l):
        for t0 in (0, 8):
            low = zero
            for k in range(16 + t0, KERNEL):
                low = low + tap(k, l) * tail[l, pl.ds(31 + t0 - k, 8)]
            rows = pl.ds(t0, 8)
            back[l, rows] = back[l, rows] + low
            high = zero
            for k in range(7 + t0):
                high = high + tap(k, l) * tail[l, pl.ds(31 + t0 - k, 8)]
            rows = pl.ds(OUT_PITCH * 7 + 16 + t0, 8)
            back[l, rows] = back[l, rows] + high

    phase("outputs")

    @pl.loop(0, SUB)
    def _(s):
        for half in range(2):
            rows = pl.ds(pl.multiple_of(32 * s + 16 * half, 16), 16)
            for l in range(LANES):
                lanes = slice(128 * l, 128 * l + 128)
                g = back[l, pl.ds(pl.multiple_of(OUT_PITCH * s + 16 * half, 8), 16)]
                sig = sigmoid(gate[rows, lanes].astype(F32))
                d_value[rows, lanes] = (g * sig).astype(BF16)
                d_gate[rows, lanes] = (
                    g * value[rows, lanes].astype(F32) * sig * (1.0 - sig)
                ).astype(BF16)

    phase("rs_wait")
    scale = 1.0 / math.sqrt(total)
    phase("z_wait")

    @pl.when(t == ADDER)
    def _():
        arrived(line, nz, z_send, z_recv)
        one, two = line[0, 0], line[0, 1]
        for i in range(1, nz):
            one, two = one + line[i, 0], two + line[i, 1]
        final[mine] = two * scale
        other[...] = one * scale
        for device in in_plane:
            exchange(other, final.at[mine], ag_send, ag_recv, core(device, 1 - ADDER)).start()
            exchange(
                final.at[mine], final.at[mine], ag_send, ag_recv, core(device, ADDER)
            ).start()
        exchange(other, final.at[mine], ag_send, ag_recv, partner).start()

    phase("shift_wait")
    d_shift[...] = from_axis(shift_z, nz, 2) * scale
    phase("ag_wait")

    @pl.when(t == ADDER)
    def _():
        taken(ag_recv, plane - 1)
        taken(ag_send, 2 * plane - 1)
        taken(rs_send, plane - 1)

    @pl.when(t != ADDER)
    def _():
        taken(ag_recv, plane)
        taken(rs_send, plane)

    phase("finish")
    for g in range(4):
        for l in range(LANES):
            lanes = slice(128 * l, 128 * l + 128)
            if g < 3:
                d_taps[8 * g : 8 * g + 8, lanes] = final[g * LANES + l]
            else:
                last = final[g * LANES + l]
                d_taps[24:KERNEL, lanes] = last[:7]
                d_gain[:, lanes] = last[7:]
    phase(None)


def shards(dims, total, value_in, gate_in, taps, gain, shift, w_out, grad_out):
    nz, ny, nx = dims
    depth = grad_out.shape[1]
    vmem = pltpu.VMEM
    dma = pltpu.SemaphoreType.DMA
    padded = (LANES, 10 * PITCH, 128)
    rows = (LANES, ROWS, 128)
    spread = (LANES, SUB * OUT_PITCH, 128)
    scratch = [
        vmem((ROWS, WIDTH), BF16), vmem((ROWS, WIDTH), BF16), vmem((KERNEL, WIDTH), F32),
        vmem((1, WIDTH), F32), vmem((1, WIDTH), F32), vmem((WIDTH, depth), BF16),
        vmem((ROWS, depth), BF16),
        vmem(padded, F32), vmem(rows, F32), vmem(spread, F32), vmem(rows, F32),
        vmem(padded, F32), vmem(spread, F32), vmem(rows, F32), vmem((8, 128), F32),
        vmem((2, 16, WIDTH), BF16), vmem((2, 16, WIDTH), BF16), vmem((LANES, 48, 128), F32),
        vmem((2, LANES, 16, 128), F32), vmem((2, LANES, 16, 128), F32),
        vmem((LANES, 48, 128), F32),
        vmem((2, 2, SUB, 128), F32), vmem((2, 2, SUB, 128), F32),
        vmem((ROWS, 128), F32), vmem((ROWS, 128), F32), vmem((ROWS, 128), F32),
        vmem((ROWS, 128), F32), vmem((ROWS, 128), F32), vmem((ROWS, 128), F32),
        vmem((32, 8, 128), F32), vmem((64, 8, 128), F32), vmem((nz, 2, 8, 128), F32),
        vmem((32, 8, 128), F32), vmem((8, 128), F32), vmem((nx, 8, 128), F32), vmem((ny, 8, 128), F32),
        vmem((nz, 8, 128), F32), vmem((64, 128), F32),
        dma((6,)), dma((4,)), dma((2,)), dma((2,)), dma((2,)), dma((2,)), dma((2,)), dma((2,)),
        dma, dma, dma, dma, dma, dma, dma((3,)), dma((3,)),
        pltpu.SemaphoreType.REGULAR((ROUNDS,)),
    ]
    hbm = pl.BlockSpec(memory_space=pltpu.HBM)
    near = pl.BlockSpec(memory_space=pltpu.VMEM)
    shape = jax.ShapeDtypeStruct
    shapes = (
        shape((ROWS, WIDTH), BF16), shape((ROWS, WIDTH), BF16), shape((KERNEL, WIDTH), F32),
        shape((1, WIDTH), F32), shape((8, 128), F32),
    )
    results = pl.pallas_call(
        functools.partial(kernel, dims, total),
        out_shape=shapes,
        in_specs=[hbm] * 7,
        out_specs=(near,) * 5,
        scratch_shapes=scratch,
        compiler_params=pltpu.CompilerParams(
            collective_id=0, has_side_effects=True, vmem_limit_bytes=40 * 2**20
        ),
        name="module",
    )(*(pltpu.with_memory_space_constraint(a, pltpu.HBM) for a in (value_in, gate_in, taps, gain.reshape(1, WIDTH), shift.reshape(1, WIDTH), w_out, grad_out)))
    d_value, d_gate, d_taps, d_gain, d_shift = pl.pallas_call(
        put_out,
        out_shape=shapes,
        in_specs=[pl.BlockSpec(memory_space=pl.ANY)] * 5,
        out_specs=(hbm,) * 5,
        scratch_shapes=[dma((5,))],
        compiler_params=pltpu.CompilerParams(vmem_limit_bytes=2**20),
        name="put_out",
    )(*results)
    return d_value, d_gate, d_taps, d_gain.reshape(WIDTH), d_shift.reshape(WIDTH)


def put_out(*refs):
    sems = refs[10]
    copies = [pltpu.make_async_copy(refs[i], refs[5 + i], sems.at[i]) for i in range(5)]
    for copy in copies:
        copy.start()
    for copy in copies:
        copy.wait()


def solution(mesh, dims=(12, 8, 4)):
    finer = Mesh(mesh.devices.reshape(*dims, mesh.shape["tp"]), (*SP, "tp"))
    total = ROWS * math.prod(dims)
    return jax.shard_map(
        functools.partial(shards, dims, total),
        mesh=finer,
        in_specs=(
            P(SP, "tp"), P(SP, "tp"), P(None, "tp"), P("tp"), P("tp"), P("tp", None), P(SP, None),
        ),
        out_specs=(P(SP, "tp"), P(SP, "tp"), P(None, "tp"), P("tp"), P("tp")),
        check_vma=False,
    )
```
